512 devices in a mesh: grp: 2 (over y), sp: 64 (over z, core), tp: 4 (over x).
Axes of the slice: x: 4, y: 2, z: 32, core: 2. Of those that a mesh axis runs over, the one named last changes fastest.
The devices are a block of a 4x8x32 slice.
Arguments:
- tokens: bfloat16 [65536, 2048], P(('grp', 'sp', 'tp')), parts along dimension 0, may hold values from -6 to 6
- norm_gain: bfloat16 [2048], replicated, may hold values from 0.099609375 to 1.8984375
- conv_outer_weight: bfloat16 [2048, 1024], P('sp', 'tp'), may hold values from -0.125 to 0.125
- conv_inner_weight: bfloat16 [2048, 1024], P('sp', 'tp'), may hold values from -0.125 to 0.125
- conv_input_weight: bfloat16 [2048, 1024], P('sp', 'tp'), may hold values from -0.125 to 0.125
- query_matrix: bfloat16 [2048, 1024], P('sp', 'tp'), may hold values from -0.125 to 0.125
- key_weight: bfloat16 [2048, 1024], P('sp', 'tp'), may hold values from -0.125 to 0.125
- value_weight: bfloat16 [2048, 1024], P('sp', 'tp'), may hold values from -0.125 to 0.125
- gate_weight: bfloat16 [2048, 1024], P('sp', 'tp'), may hold values from -0.125 to 0.125
- conv_taps: bfloat16 [3, 1024], P(None, 'tp'), may hold values from -3.5 to 3.5
- conv_out_weight: bfloat16 [1024, 2048], P('tp', 'sp'), may hold values from -0.125 to 0.125
- ret_out_weight: bfloat16 [1024, 2048], P('tp', 'sp'), may hold values from -0.125 to 0.125
- log_decay: float32 [65536, 8], P(('grp', 'sp'), 'tp'), parts along dimension 0, may hold values from -0.75 to 0
Outputs:
- mixed: bfloat16 [65536, 2048], P(('grp', 'sp', 'tp')), parts along dimension 0
The draws below stay inside these ranges and needn't reach their ends.
There are 2 independent parts, one for each index of `grp`. The reference program is written for one: setup_inputs(seed, part) draws one part's arguments, and reference() takes and returns one part's arrays. A program takes and returns all parts, laid end to end along the dimension named above; an argument that names none is the same for every part. Nothing has to cross between parts.
All inputs are finite; a program needn't handle non-finite values.
Results may differ from the reference program's by a relative error of at most 0.025.
Values may be sent and summed in bfloat16 or wider, within the bound.
No kernel may reach another device: no remote copies, remote signals or barrier semaphores. Data moves between devices by JAX's collectives and lax.ppermute only.
A program may use at most 64 MiB of HBM per device.

```python
import math
import jax
import jax.numpy as jnp
from jax import lax

D = 2048
CONV_W = 1024
RET_HEADS = 8
HEAD = 128
CONV_K = 3
BLOCK = 128
TOK_SP = 512
RET_W = 1024
SEQUENCE_TOKENS = 32768
N_TP = 4


def draw_log_decay(key, part):
    folded = jax.random.fold_in(key, 17)
    random_subkeys = jax.random.split(folded, 7)
    ranking = jax.random.permutation(random_subkeys[0], RET_HEADS)
    fast_count = RET_HEADS // 2
    is_fast = (ranking < fast_count).astype(jnp.float32)
    fast_rate = jnp.exp(jax.random.uniform(random_subkeys[1], (RET_HEADS,), jnp.float32, math.log(1.0 / 100.0), math.log(1.0 / 30.0)))
    slow_rate = jnp.exp(jax.random.uniform(random_subkeys[2], (RET_HEADS,), jnp.float32, math.log(0.02), math.log(0.3))) / SEQUENCE_TOKENS
    rates = is_fast * fast_rate + (1.0 - is_fast) * slow_rate
    span_count = SEQUENCE_TOKENS // TOK_SP
    span_factor = jnp.exp(jax.random.uniform(random_subkeys[3], (span_count,), jnp.float32, math.log(0.5), math.log(2.0)))
    span_index = jnp.arange(SEQUENCE_TOKENS, dtype=jnp.int32) // TOK_SP
    position_factor = span_factor[span_index]
    jitter = jax.random.uniform(random_subkeys[4], (SEQUENCE_TOKENS, RET_HEADS), jnp.float32, 0.5, 1.5)
    decay_values = -rates[None, :] * position_factor[:, None] * jitter
    spike_position = jax.random.permutation(random_subkeys[5], SEQUENCE_TOKENS)[:3].astype(jnp.int32)
    spike_log_decay = jnp.log(jax.random.uniform(random_subkeys[6], (3,), jnp.float32, 0.55, 0.8))
    spike_reached = (jnp.arange(SEQUENCE_TOKENS, dtype=jnp.int32)[:, None] == spike_position[None, :]).astype(jnp.float32)
    decay_values = decay_values + jnp.sum(spike_reached * spike_log_decay[None, :], axis=1)[:, None]
    return decay_values.astype(jnp.float32)


def level_of(key, dims, shards, smallest, high):
    gain, own = 1.0, jax.random.fold_in(key, 6)
    for axis_at, parts in shards:
        heights = jnp.exp(jax.random.uniform(jax.random.fold_in(own, axis_at), (parts,), jnp.float32, smallest / len(shards), high / len(shards)))
        gain = gain * jnp.repeat(heights, dims[axis_at] // parts).reshape([-1 if axis == axis_at else 1 for axis in range(len(dims))])
    return gain


def normal_values(key, dims, scale, limit, cuts=(), kind=jnp.bfloat16):
    entries = jax.random.normal(key, dims, jnp.float32) * scale
    if len(cuts) > 0:
        entries = level_of(key, dims, cuts, -0.22, 0.18) * entries
    return jnp.clip(entries, min=-limit, max=limit).astype(kind)


def setup_inputs(seed: int = 0, part: int = 0) -> dict:
    seeds = jax.random.split(jax.random.key(seed), 14)
    part_keys = jax.random.split(jax.random.fold_in(seeds[13], part), 14)
    tokens = normal_values(part_keys[0], (SEQUENCE_TOKENS, D), 1.0, 6.0, ((0, 256),))
    norm_gain = jnp.clip(1.0 + 0.18 * jax.random.normal(seeds[1], (D,), jnp.float32), 0.099609375, 1.8984375).astype(jnp.bfloat16)
    conv_outer_weight = normal_values(seeds[2], (D, CONV_W), D ** -0.5, 0.125, ((0, 64), (1, 4)))
    conv_inner_weight = normal_values(seeds[3], (D, CONV_W), D ** -0.5, 0.125, ((0, 64), (1, 4)))
    conv_input_weight = normal_values(seeds[4], (D, CONV_W), D ** -0.5, 0.125, ((0, 64), (1, 4)))
    query_matrix = normal_values(seeds[5], (D, RET_W), D ** -0.5, 0.125, ((0, 64), (1, 4)))
    key_weight = normal_values(seeds[6], (D, RET_W), D ** -0.5, 0.125, ((0, 64), (1, 4)))
    value_weight = normal_values(seeds[7], (D, RET_W), D ** -0.5, 0.125, ((0, 64), (1, 4)))
    gate_weight = normal_values(seeds[8], (D, RET_W), D ** -0.5, 0.125, ((0, 64), (1, 4)))
    conv_taps = normal_values(seeds[9], (CONV_K, CONV_W), CONV_K ** -0.5, 3.5, ((1, 4),))
    conv_out_weight = normal_values(seeds[10], (CONV_W, D), (CONV_W + RET_W) ** -0.5, 0.125, ((0, 4), (1, 64)))
    ret_out_weight = normal_values(seeds[11], (RET_W, D), (CONV_W + RET_W) ** -0.5, 0.125, ((0, 4), (1, 64)))
    log_decay = draw_log_decay(jax.random.fold_in(jax.random.fold_in(seeds[13], part), 71), part)
    return {"tokens": tokens, "norm_gain": norm_gain, "conv_outer_weight": conv_outer_weight, "conv_inner_weight": conv_inner_weight, "conv_input_weight": conv_input_weight, "query_matrix": query_matrix, "key_weight": key_weight, "value_weight": value_weight, "gate_weight": gate_weight, "conv_taps": conv_taps, "conv_out_weight": conv_out_weight, "ret_out_weight": ret_out_weight, "log_decay": log_decay}


EPSILON = 1e-06
ROTARY_BASE = 10000.0
HIGHEST_PRECISION = lax.Precision.HIGHEST

def rotate(head_data, positions):
    half_width = head_data.shape[-1] // 2
    inv_freq = ROTARY_BASE ** (-jnp.arange(half_width, dtype=jnp.float32) / half_width)
    angles = positions[:, None] * inv_freq[None, :]
    cosine = jnp.cos(angles)[:, None, :]
    sine_part = jnp.sin(angles)[:, None, :]
    first_half = head_data[..., :half_width]
    second_half = head_data[..., half_width:]
    return jnp.concatenate([first_half * cosine - second_half * sine_part, second_half * cosine + first_half * sine_part], axis=-1)

def head_norm(head_data):
    return head_data * lax.rsqrt(lax.optimization_barrier(jnp.mean(head_data * head_data, axis=-1, keepdims=True)) + EPSILON)

def retain(queries, keys_rot, head_values, log_decay):
    block_count = SEQUENCE_TOKENS // BLOCK
    block_shape = (block_count, BLOCK, RET_HEADS, HEAD)
    offsets = jnp.arange(BLOCK, dtype=jnp.int32)
    causal_mask = (offsets[:, None] >= offsets[None, :])[:, :, None]

    def block_step(carried, pieces):
        query_block, key_block, value_block, log_block = pieces
        cumulative = jnp.cumsum(log_block, axis=0)
        spread = cumulative[:, None, :] - cumulative[None, :, :]
        decay_grid = jnp.where(causal_mask, jnp.exp(jnp.where(causal_mask, spread, 0.0)), 0.0)
        scores = jnp.einsum('ihd,jhd->ijh', query_block, key_block, precision=HIGHEST_PRECISION) * decay_grid
        within = jnp.einsum('ijh,jhe->ihe', scores, value_block, precision=HIGHEST_PRECISION)
        across = jnp.einsum('ihd,hde->ihe', query_block, carried, precision=HIGHEST_PRECISION)
        across = across * jnp.exp(cumulative)[:, :, None]
        block_end = cumulative[-1]
        weights = jnp.exp(block_end[None, :] - cumulative)
        increment = jnp.einsum('jh,jhd,jhe->hde', weights, key_block, value_block, precision=HIGHEST_PRECISION)
        updated = jnp.exp(block_end)[:, None, None] * carried + increment
        return (updated, within + across)
    start_state = jnp.zeros((RET_HEADS, HEAD, HEAD), jnp.float32)
    _, outputs = lax.scan(block_step, start_state, (queries.reshape(block_shape), keys_rot.reshape(block_shape), head_values.reshape(block_shape), log_decay.reshape(block_count, BLOCK, RET_HEADS)))
    return outputs.reshape(SEQUENCE_TOKENS, RET_HEADS, HEAD)

def reference(tokens, norm_gain, conv_outer_weight, conv_inner_weight, conv_input_weight, query_matrix, key_weight, value_weight, gate_weight, conv_taps, conv_out_weight, ret_out_weight, log_decay):
    values32 = tokens.astype(jnp.float32)
    normed = (values32 * lax.rsqrt(lax.optimization_barrier(jnp.mean(values32 * values32, axis=-1, keepdims=True)) + EPSILON) * norm_gain.astype(jnp.float32)).astype(jnp.bfloat16)

    def project(weight):
        return jnp.dot(normed, weight, preferred_element_type=jnp.float32).astype(jnp.bfloat16)
    conv_outer = project(conv_outer_weight)
    conv_inner = project(conv_inner_weight)
    conv_input = project(conv_input_weight)
    query_proj = project(query_matrix)
    key_proj = project(key_weight)
    value_proj = project(value_weight)
    gate_proj = project(gate_weight)
    mixed_in = conv_inner.astype(jnp.float32) * conv_input.astype(jnp.float32)
    extended = jnp.concatenate([jnp.zeros((CONV_K - 1, CONV_W), jnp.float32), mixed_in], axis=0)
    taps = conv_taps.astype(jnp.float32)
    conv_out = jnp.zeros((SEQUENCE_TOKENS, CONV_W), jnp.float32)
    for tap_index in range(CONV_K):
        conv_out = conv_out + taps[tap_index][None, :] * extended[tap_index:tap_index + SEQUENCE_TOKENS]
    conv_branch = (conv_outer.astype(jnp.float32) * conv_out).astype(jnp.bfloat16)
    positions = jnp.arange(SEQUENCE_TOKENS, dtype=jnp.float32)
    head_shape = (SEQUENCE_TOKENS, RET_HEADS, HEAD)
    queries = rotate(query_proj.astype(jnp.float32).reshape(head_shape), positions)
    keys_rot = rotate(key_proj.astype(jnp.float32).reshape(head_shape), positions) * HEAD ** (-0.5)
    head_values = value_proj.astype(jnp.float32).reshape(head_shape)
    retained = retain(queries, keys_rot, head_values, log_decay)
    ret_branch = (head_norm(retained).reshape(SEQUENCE_TOKENS, RET_W) * jax.nn.silu(gate_proj.astype(jnp.float32))).astype(jnp.bfloat16)
    conv_group = CONV_W // N_TP
    ret_group = RET_W // N_TP
    summed = jnp.zeros((SEQUENCE_TOKENS, D), jnp.float32)
    for group_index in range(N_TP):
        conv_lo = group_index * conv_group
        ret_lo = group_index * ret_group
        partial_term = jnp.dot(conv_branch[:, conv_lo:conv_lo + conv_group], conv_out_weight[conv_lo:conv_lo + conv_group], preferred_element_type=jnp.float32)
        partial_term = partial_term + jnp.dot(ret_branch[:, ret_lo:ret_lo + ret_group], ret_out_weight[ret_lo:ret_lo + ret_group], preferred_element_type=jnp.float32)
        summed = summed + partial_term.astype(jnp.bfloat16).astype(jnp.float32)
    return summed.astype(jnp.bfloat16)
```

```python
import functools

import jax
import jax.numpy as jnp
from jax import lax
from jax.experimental import pallas as pl
from jax.experimental.pallas import tpu as pltpu
from jax.sharding import Mesh, PartitionSpec as P

HEAD = 128
HALF = HEAD // 2
CONV_K = 3
EPSILON = 1e-06
ROTARY_BASE = 10000.0
BLOCK = 256
EXTRA = 16
INTERPRET = False

BF16 = jnp.bfloat16
F32 = jnp.float32
CHIPS = ("za", "zb", "zc")
NEAR = ("zb", "zc")
FAR = ("za", "zb")
PAIR = ("zc", "core")

VMEM = pl.BlockSpec(memory_space=pltpu.VMEM)
SMEM = pl.BlockSpec(memory_space=pltpu.SMEM)


def call(kernel, outs, name, n_scalar=0, scratch=(), flops=0):
    def run(*args):
        return pl.pallas_call(
            kernel,
            out_shape=outs,
            in_specs=[SMEM] * n_scalar + [VMEM] * (len(args) - n_scalar),
            out_specs=jax.tree.map(lambda _: VMEM, outs),
            scratch_shapes=list(scratch),
            interpret=INTERPRET,
            name=name,
            cost_estimate=pl.CostEstimate(flops=flops, bytes_accessed=0, transcendentals=0),
        )(*args)

    return run


def shape(dims, kind):
    return jax.ShapeDtypeStruct(dims, kind)


def dot(a, b, dims):
    return lax.dot_general(a, b, (dims, ((), ())), preferred_element_type=F32)


def pack_kernel(*refs):
    *inputs, out = refs
    for at, ref in enumerate(inputs):
        for core in range(2):
            half = ref[:, core * HEAD : (core + 1) * HEAD]
            for pair in range(2):
                out[2 * pair + core, :, at * HEAD : (at + 1) * HEAD] = half


def norm_kernel(tokens, gain, out):
    values = tokens[...].astype(F32)
    scale = lax.rsqrt(jnp.mean(values * values, axis=-1, keepdims=True) + EPSILON)
    normed = (values * scale * gain[...].astype(F32)).astype(BF16)
    for copy in range(out.shape[0]):
        out[copy] = normed


def rotated(head, cosine, sine):
    wide_cosine = jnp.concatenate([cosine, cosine], axis=-1)
    wide_sine = jnp.concatenate([-sine, sine], axis=-1)
    turned = jnp.concatenate([head[:, HALF:], head[:, :HALF]], axis=-1)
    return head * wide_cosine + turned * wide_sine


def in_three(log_total):
    high = log_total.astype(BF16).astype(F32)
    middle = (log_total - high).astype(BF16).astype(F32)
    low = log_total - high - middle
    row = lax.broadcasted_iota(jnp.int32, (EXTRA, HEAD), 0)
    rows = jnp.where(row == 0, high, jnp.where(row == 1, middle, jnp.where(row == 2, low, 0.0)))
    return rows.astype(BF16)


def from_three(rows):
    rows = rows.astype(F32)
    return rows[0:1] + rows[1:2] + rows[2:3]


def kv_kernel(x, wk, wv, cosine, sine, decay, k_out, v_out, message):
    rows = x.shape[0]
    total = decay[rows - 1 : rows, :]
    weight = jnp.concatenate([wk[...], wv[...]], axis=1)

    def block(i, state):
        at = pl.ds(pl.multiple_of(i * BLOCK, BLOCK), BLOCK)
        both = dot(x[at, :], weight, ((1,), (0,))).astype(BF16)
        key = rotated(both[:, :HEAD].astype(F32), cosine[at, :], sine[at, :]) * HEAD ** (-0.5)
        k_out[at, :] = key.astype(BF16)
        value = both[:, HEAD:]
        v_out[at, :] = value
        faded = (key * jnp.exp(total - decay[at, :])).astype(BF16)
        return state + dot(faded, value, ((0,), (0,)))

    state = lax.fori_loop(0, rows // BLOCK, block, jnp.zeros((HEAD, HEAD), F32))
    extra = in_three(jnp.broadcast_to(total, (1, HEAD)))
    for copy in range(message.shape[0]):
        message[copy, :HEAD, :] = state.astype(BF16)
        message[copy, HEAD:, :] = extra


def near_kernel(place, gathered, message, before, fade, scratch):
    own = place[0]
    run = jnp.zeros((HEAD, HEAD), F32)
    passed = jnp.zeros((1, HEAD), F32)
    kept, kept_passed = run, passed
    for at in range(gathered.shape[0]):
        kept = jnp.where(own == at, run, kept)
        kept_passed = jnp.where(own == at, passed, kept_passed)
        log_total = from_three(gathered[at, HEAD:, :])
        run = jnp.exp(log_total) * run + gathered[at, :HEAD, :].astype(F32)
        passed = passed + log_total
    before[...] = kept
    fade[...] = jnp.broadcast_to(jnp.exp(kept_passed), fade.shape)
    scratch[...] = run
    share = HEAD // gathered.shape[0]
    part = scratch[pl.ds(pl.multiple_of(own * share, share), share), :].astype(BF16)
    extra = in_three(passed)
    for copy in range(message.shape[0]):
        message[copy, :share, :] = part
        message[copy, share:, :] = extra


def far_kernel(place, gathered, message):
    own = place[0]
    share = message.shape[1]
    run = jnp.zeros((share, HEAD), F32)
    kept = run
    for at in range(gathered.shape[0]):
        kept = jnp.where(own == at, run, kept)
        run = jnp.exp(from_three(gathered[at, share:, :])) * run + gathered[at, :share, :].astype(F32)
    for copy in range(message.shape[0]):
        message[copy] = kept.astype(BF16)


def branch_kernel(
    core, x, halo, weights, cosine, sine, decay, decay_row, keys, values, base, before, fade, taps, keep, send
):
    rows = x.shape[0]
    own = core[0]
    share = base.shape[1]
    parts = [base[at].astype(F32) for at in range(base.shape[0])]
    incoming = fade[0:1, :] * jnp.concatenate(parts, axis=0) + before[...]
    weight = weights[:, : 5 * HEAD]
    rim = dot(halo[...], weights[:, HEAD : 3 * HEAD], ((1,), (0,))).astype(BF16).astype(F32)
    tail = (rim[:, :HEAD] * rim[:, HEAD:])[EXTRA - 8 :]
    row = lax.broadcasted_iota(jnp.int32, (BLOCK, HEAD), 0)
    causal = lax.broadcasted_iota(jnp.int32, (BLOCK, BLOCK), 0) >= lax.broadcasted_iota(
        jnp.int32, (BLOCK, BLOCK), 1
    )
    tap = taps[...].astype(F32)
    state = incoming
    start = jnp.zeros((1, 1), F32)
    for i in range(rows // BLOCK):
        at = pl.ds(i * BLOCK, BLOCK)
        projected = dot(x[at, :], weight, ((1,), (0,))).astype(BF16)
        outer = projected[:, :HEAD].astype(F32)
        mixed = projected[:, HEAD : 2 * HEAD].astype(F32) * projected[:, 2 * HEAD : 3 * HEAD].astype(F32)
        one = jnp.where(row == 0, tail[7:8], pltpu.roll(mixed, 1, 0))
        two = jnp.where(row == 0, tail[6:7], jnp.where(row == 1, tail[7:8], pltpu.roll(mixed, 2, 0)))
        conv = tap[0:1] * two + tap[1:2] * one + tap[2:3] * mixed
        tail = mixed[BLOCK - 8 :]
        conv_branch = (outer * conv).astype(BF16)

        query = rotated(projected[:, 3 * HEAD : 4 * HEAD].astype(F32), cosine[at, :], sine[at, :])
        query16 = query.astype(BF16)
        key, value = keys[at, :], values[at, :]
        column = decay[at, :]
        line = decay_row[:, i * BLOCK : (i + 1) * BLOCK]
        spread = jnp.where(causal, column - line, 0.0)
        scores = jnp.where(causal, dot(query16, key, ((1,), (1,))) * jnp.exp(spread), 0.0)
        within = dot(scores.astype(BF16), value, ((1,), (0,)))
        across = dot(query16, state.astype(BF16), ((1,), (0,))) * jnp.exp(column - start)
        retained = within + across
        end = decay[(i + 1) * BLOCK - 1 : (i + 1) * BLOCK, :]
        faded = (key.astype(F32) * jnp.exp(end - column)).astype(BF16)
        state = jnp.exp(end - start) * state + dot(faded, value, ((0,), (0,)))
        start = end
        normed = retained * lax.rsqrt(jnp.mean(retained * retained, axis=-1, keepdims=True) + EPSILON)
        gate = projected[:, 4 * HEAD :].astype(F32)
        ret_branch = (normed * (gate / (1.0 + jnp.exp(-gate)))).astype(BF16)

        half = (i * BLOCK) // (rows // 2)
        place = pl.ds(i * BLOCK - half * (rows // 2), BLOCK)

        @pl.when(own == half)
        def _():
            keep[place, :HEAD] = conv_branch
            keep[place, HEAD:] = ret_branch

        @pl.when(own != half)
        def _():
            send[place, :HEAD] = conv_branch
            send[place, HEAD:] = ret_branch


def out_kernel(mine, theirs, own_weight, other_weight, out):
    parts, rows = out.shape[0], out.shape[1]
    step = 512
    for column in range(0, out.shape[2], step):
        at = pl.ds(column, step)
        total = dot(mine[...], own_weight[at, :], ((1,), (1,))) + dot(theirs[...], other_weight[at, :], ((1,), (1,)))
        total = total.astype(BF16)
        for part in range(parts):
            out[part, :, column : column + step] = total[part * rows : (part + 1) * rows]


def sum_kernel(parts, out):
    total = parts[0].astype(F32)
    for at in range(1, parts.shape[0]):
        total = total + parts[at].astype(F32)
    out[...] = total.astype(BF16)


def exchanged(x, axes):
    return lax.all_to_all(x, axes, 0, 0, tiled=True)


def body(
    tokens,
    norm_gain,
    conv_outer_weight,
    conv_inner_weight,
    conv_input_weight,
    query_matrix,
    key_weight,
    value_weight,
    gate_weight,
    conv_taps,
    conv_out_weight,
    ret_out_weight,
    log_decay,
):
    own_rows, width = tokens.shape
    tp = lax.axis_size("tp")
    chip = lax.axis_index(CHIPS)
    core = lax.axis_index("core")
    chips = lax.axis_size(CHIPS)
    near, far = lax.axis_size(NEAR), lax.axis_size("za")
    rows = 2 * tp * own_rows
    shard = key_weight.shape[0]

    packed = call(pack_kernel, shape((4, shard, 9 * HEAD), BF16), "pack")(
        key_weight,
        value_weight,
        conv_outer_weight,
        conv_inner_weight,
        conv_input_weight,
        query_matrix,
        gate_weight,
        conv_out_weight.T,
        ret_out_weight.T,
    )
    bundle = exchanged(packed, PAIR).reshape(4 * shard, 9 * HEAD)
    rest = lax.all_gather(bundle[:, 2 * HEAD :], FAR, axis=0, tiled=True)
    wk = lax.all_gather(bundle[:, :HEAD], FAR).reshape(width, HEAD)
    wv = lax.all_gather(bundle[:, HEAD : 2 * HEAD], FAR).reshape(width, HEAD)

    normed = call(norm_kernel, shape((2 * tp, own_rows, width), BF16), "norm")(
        tokens, norm_gain.reshape(1, width)
    )
    x = exchanged(normed, ("core", "tp")).reshape(rows, width)
    halo = lax.ppermute(x[rows - EXTRA :], CHIPS, [(i, i + 1) for i in range(chips - 1)])

    logs = exchanged(log_decay.T, "core").reshape(rows // HEAD, HEAD)
    upper = jnp.triu(jnp.ones((HEAD, HEAD), F32))
    inner = jnp.dot(logs, upper, precision=lax.Precision.HIGHEST)
    ends = inner[:, -1]
    lower = jnp.tril(jnp.ones((rows // HEAD, rows // HEAD), F32), -1)
    cumulative = inner + jnp.sum(lower * ends[None, :], axis=1)[:, None]
    decay = cumulative.reshape(rows, 1)
    decay_row = cumulative.reshape(1, rows)

    positions = (chip * rows).astype(F32) + jnp.arange(rows, dtype=F32)
    inv_freq = ROTARY_BASE ** (-jnp.arange(HALF, dtype=F32) / HALF)
    angles = positions[:, None] * inv_freq[None, :]
    cosine, sine = jnp.cos(angles), jnp.sin(angles)

    keys, values, message = call(
        kv_kernel,
        (shape((rows, HEAD), BF16), shape((rows, HEAD), BF16), shape((near, HEAD + EXTRA, HEAD), BF16)),
        "kv",
        flops=4 * rows * width * HEAD,
    )(x, wk, wv, cosine, sine, decay)

    share = HEAD // near
    gathered = exchanged(message, NEAR)
    message, before, fade = call(
        near_kernel,
        (shape((far, share + EXTRA, HEAD), BF16), shape((HEAD, HEAD), F32), shape((8, HEAD), F32)),
        "near",
        n_scalar=1,
        scratch=[pltpu.VMEM((HEAD, HEAD), F32)],
    )(lax.axis_index(NEAR).reshape(1), gathered)
    gathered = exchanged(message, "za")
    message = call(far_kernel, shape((near, share, HEAD), BF16), "far", n_scalar=1)(
        lax.axis_index("za").reshape(1), gathered
    )
    base = exchanged(message, NEAR)

    other_core = [(0, 1), (1, 0)]
    out_own = rest[:, 5 * HEAD :]
    out_other = lax.ppermute(out_own, "core", other_core)
    keep, send = call(
        branch_kernel,
        (shape((rows // 2, 2 * HEAD), BF16), shape((rows // 2, 2 * HEAD), BF16)),
        "branch",
        n_scalar=1,
        flops=10 * rows * width * HEAD,
    )(
        core.reshape(1),
        x,
        halo,
        rest,
        cosine,
        sine,
        decay,
        decay_row,
        keys,
        values,
        base,
        before,
        fade,
        lax.dynamic_slice_in_dim(conv_taps, core * HEAD, HEAD, 1),
    )
    theirs = lax.ppermute(send, "core", other_core)
    partial = call(out_kernel, shape((tp, own_rows, width), BF16), "out", flops=rows * width * 4 * HEAD)(
        keep, theirs, out_own, out_other
    )
    return call(sum_kernel, shape((own_rows, width), BF16), "sum")(exchanged(partial, "tp"))


def solution(mesh):
    groups, stretches, tp = mesh.devices.shape
    chips = stretches // 2
    fine = Mesh(
        mesh.devices.reshape(groups, chips // 4, 2, 2, 2, tp), ("grp", "za", "zb", "zc", "core", "tp")
    )
    sp = ("za", "zb", "zc", "core")
    columns = P(sp, "tp")
    placed = (
        P(("grp", *sp, "tp"), None),
        P(),
        *([columns] * 7),
        P(None, "tp"),
        P("tp", sp),
        P("tp", sp),
        P(("grp", *sp), "tp"),
    )
    return jax.shard_map(
        body, mesh=fine, in_specs=placed, out_specs=P(("grp", *sp, "tp"), None), check_vma=False
    )
```

```python
import jax
import jax.numpy as jnp
from jax import lax
from jax.experimental import pallas as pl
from jax.experimental.pallas import tpu as pltpu
from jax.sharding import Mesh, PartitionSpec as P

HEAD = 128
HALF = HEAD // 2
CONV_K = 3
EPSILON = 1e-06
ROTARY_BASE = 10000.0
BLOCK = 256
EXTRA = 16
PROJECTED = 5 * HEAD
COLUMNS = 7 * HEAD
INTERPRET = False

BF16 = jnp.bfloat16
F32 = jnp.float32
CHIPS = ("za", "zb", "zc")
STRETCHES = ("za", "zb", "zc", "core")
NEAR = ("zb", "zc")
FAR = ("za", "zb")

VMEM = pl.BlockSpec(memory_space=pltpu.VMEM)
PLAIN = pl.BlockSpec(memory_space=pltpu.VMEM)
SMEM = pl.BlockSpec(memory_space=pltpu.SMEM)
ANY = pl.BlockSpec(memory_space=pl.ANY)


def call(kernel, outs, name, specs=None, scratch=(), flops=0, limit=16):
    def run(*args):
        in_specs = specs if specs is not None else [VMEM] * len(args)
        placed = [placed_for(arg, spec) for arg, spec in zip(args, in_specs)]
        return pl.pallas_call(
            kernel,
            out_shape=[o[0] for o in outs],
            in_specs=in_specs,
            out_specs=[o[1] for o in outs],
            scratch_shapes=list(scratch),
            interpret=INTERPRET,
            name=name,
            compiler_params=pltpu.CompilerParams(vmem_limit_bytes=limit << 20 if limit else None),
            cost_estimate=pl.CostEstimate(flops=flops, bytes_accessed=0, transcendentals=0),
        )(*placed)

    return run


def placed_for(arg, spec):
    if INTERPRET or all(spec is not kind for kind in (VMEM, ANY)):
        return arg
    return pltpu.with_memory_space_constraint(arg, pltpu.VMEM if spec is VMEM else pltpu.HBM)


def fast(dims, kind):
    return (jax.ShapeDtypeStruct(dims, kind) if INTERPRET else pltpu.VMEM(dims, kind), VMEM)


def slow(dims, kind):
    return (jax.ShapeDtypeStruct(dims, kind), VMEM)


def dot(a, b, dims):
    return lax.dot_general(a, b, (dims, ((), ())), preferred_element_type=F32)


def pack_kernel(key, value, *refs):
    *inputs, logs, rest, message = refs
    for at, ref in enumerate(inputs):
        for core in range(2):
            to = core * COLUMNS + at * HEAD
            rest[:, to : to + HEAD] = ref[:, core * HEAD : (core + 1) * HEAD]
    shard = key.shape[0]
    for core in range(2):
        message[core, :shard, :HEAD] = key[:, core * HEAD : (core + 1) * HEAD]
        message[core, :shard, HEAD:] = value[:, core * HEAD : (core + 1) * HEAD]
        lines = [logs[core : core + 1, at : at + 2 * HEAD] for at in range(0, logs.shape[1], 2 * HEAD)]
        line = jnp.concatenate(lines, axis=0)
        high = line.astype(BF16).astype(F32)
        middle = (line - high).astype(BF16).astype(F32)
        low = line - high - middle
        filler = jnp.zeros((EXTRA - 3 * len(lines), 2 * HEAD), F32)
        message[core, shard:, :] = jnp.concatenate([high, middle, low, filler], axis=0).astype(BF16)


def logs_of(rows, lines):
    rows = rows.astype(F32)
    return rows[:lines] + rows[lines : 2 * lines] + rows[2 * lines : 3 * lines]


def norm_kernel(tokens, gain, out):
    values = tokens[...].astype(F32)
    scale = lax.rsqrt(jnp.mean(values * values, axis=-1, keepdims=True) + EPSILON)
    normed = (values * scale * gain[...].astype(F32)).astype(BF16)
    for copy in range(out.shape[0]):
        out[copy] = normed


def rotated(head, cosine, sine):
    return head * cosine + pltpu.roll(head, HALF, 1) * sine


def kv_kernel(
    x, gathered, own, cos_far, sin_far, cos_near, sin_near, k_out, v_out, cosine, sine, decay, column, totals, message, weight
):
    rows, width = x.shape[0] * x.shape[1], x.shape[2]
    pairs, fars = gathered.shape[:2]
    shard = own.shape[1] - EXTRA
    lines = rows // 2 // (2 * HEAD)

    pieces = []
    for core in range(2):
        logs = logs_of(own[core, shard:, :], lines)
        for line in range(lines):
            pieces += [logs[line : line + 1, :HEAD], logs[line : line + 1, HEAD:]]
    logs = jnp.concatenate(pieces, axis=0)
    upper = lax.broadcasted_iota(jnp.int32, (HEAD, HEAD), 0) <= lax.broadcasted_iota(jnp.int32, (HEAD, HEAD), 1)
    inner = lax.dot_general(
        logs,
        upper.astype(F32),
        (((1,), (0,)), ((), ())),
        precision=lax.Precision.HIGHEST,
        preferred_element_type=F32,
    )
    before = jnp.zeros((1, 1), F32)
    added = []
    for at in range(len(pieces)):
        added.append(inner[at : at + 1] + before)
        before = before + inner[at : at + 1, HEAD - 1 :]
    cumulative = jnp.concatenate(added, axis=0)
    decay[...] = cumulative
    filler = jnp.zeros((HEAD - len(pieces), HEAD), F32)
    column[...] = jnp.concatenate([cumulative, filler], axis=0).T
    total = before

    for far in range(fars):
        for pair in range(pairs):
            chip = far * pairs + pair
            log_total = jnp.zeros((1, 1), F32)
            for core in range(2):
                at = core * (shard + EXTRA)
                weight[(2 * chip + core) * shard : (2 * chip + core + 1) * shard, :] = gathered[
                    pair, far, at : at + shard, :
                ]
                logs = logs_of(gathered[pair, far, at + shard : at + shard + EXTRA, :], lines)
                log_total = log_total + jnp.sum(logs, axis=(0, 1), keepdims=True)
            totals[chip : chip + 1, :] = jnp.broadcast_to(log_total, (1, HEAD))

    state = jnp.zeros((HEAD, HEAD), F32)
    for i in range(rows // BLOCK):
        at = pl.ds(i * BLOCK, BLOCK)
        cos_at = cos_far[i : i + 1, :] * cos_near[...] - sin_far[i : i + 1, :] * sin_near[...]
        sin_at = sin_far[i : i + 1, :] * cos_near[...] + cos_far[i : i + 1, :] * sin_near[...]
        first = lax.broadcasted_iota(jnp.int32, sin_at.shape, 1) < HALF
        sin_at = jnp.where(first, -sin_at, sin_at)
        cosine[at, :] = cos_at
        sine[at, :] = sin_at
        both = dot(block_rows(x, i), weight[...], ((1,), (0,))).astype(BF16)
        key = rotated(both[:, :HEAD].astype(F32), cos_at, sin_at) * HEAD ** (-0.5)
        k_out[at, :] = key.astype(BF16)
        value = both[:, HEAD:]
        v_out[at, :] = value
        here = block_column(column, i)
        faded = (key * jnp.exp(total - here)).astype(BF16)
        state = state + dot(faded, value, ((0,), (0,)))
    for copy in range(message.shape[0]):
        message[copy] = state.astype(BF16)


def block_rows(x, i):
    per = BLOCK // x.shape[1]
    return x[i * per : (i + 1) * per].reshape(BLOCK, x.shape[2])


def block_column(column, i):
    per = BLOCK // HEAD
    return jnp.concatenate([column[:, per * i + j : per * i + j + 1] for j in range(per)], axis=0)


def near_kernel(place, block, totals, gathered, message, before, fade, scratch):
    own = place[0]
    near = gathered.shape[0]
    run = jnp.zeros((HEAD, HEAD), F32)
    passed = jnp.zeros((1, HEAD), F32)
    kept, kept_passed = run, passed
    for at in range(near):
        kept = jnp.where(own == at, run, kept)
        kept_passed = jnp.where(own == at, passed, kept_passed)
        log_total = totals[pl.ds(block[0] * near + at, 1), :]
        run = jnp.exp(log_total) * run + gathered[at].astype(F32)
        passed = passed + log_total
    before[...] = kept
    fade[...] = jnp.broadcast_to(jnp.exp(kept_passed), fade.shape)
    scratch[...] = run
    share = HEAD // near
    part = scratch[pl.ds(pl.multiple_of(own * share, share), share), :].astype(BF16)
    for copy in range(message.shape[0]):
        message[copy] = part


def far_kernel(place, totals, gathered, message):
    own = place[0]
    near, share = message.shape[:2]
    run = jnp.zeros((share, HEAD), F32)
    kept = run
    for at in range(gathered.shape[0]):
        kept = jnp.where(own == at, run, kept)
        log_total = jnp.sum(totals[at * near : (at + 1) * near, :], axis=0, keepdims=True)
        run = jnp.exp(log_total) * run + gathered[at].astype(F32)
    for copy in range(near):
        message[copy] = kept.astype(BF16)


def branch_kernel(
    core,
    weights,
    x,
    halo,
    cosine,
    sine,
    decay,
    column,
    keys,
    values,
    base,
    before,
    fade,
    taps,
    keep,
    send,
    out_weight,
    weight,
    semaphores,
):
    rows = x.shape[0] * x.shape[1]
    own = core[0]
    start_at = pl.multiple_of(own * COLUMNS, HEAD)
    other_at = pl.multiple_of((1 - own) * COLUMNS, HEAD)
    copies = [
        pltpu.make_async_copy(weights.at[:, pl.ds(start_at, PROJECTED)], weight, semaphores.at[0]),
        pltpu.make_async_copy(
            weights.at[:, pl.ds(start_at + PROJECTED, 2 * HEAD)], out_weight.at[0], semaphores.at[1]
        ),
        pltpu.make_async_copy(
            weights.at[:, pl.ds(other_at + PROJECTED, 2 * HEAD)], out_weight.at[1], semaphores.at[2]
        ),
    ]
    for copy in copies:
        copy.start()
    incoming = jnp.concatenate([base[at].astype(F32) for at in range(base.shape[0])], axis=0)
    state = fade[0:1, :] * incoming + before[...]
    row = lax.broadcasted_iota(jnp.int32, (BLOCK, HEAD), 0)
    causal = lax.broadcasted_iota(jnp.int32, (BLOCK, BLOCK), 0) >= lax.broadcasted_iota(
        jnp.int32, (BLOCK, BLOCK), 1
    )
    tap = jnp.where(own == 0, taps[:, :HEAD].astype(F32), taps[:, HEAD:].astype(F32))
    start = jnp.zeros((1, 1), F32)
    per = BLOCK // HEAD
    copies[0].wait()
    rim = dot(halo[...], weight[:, HEAD : 3 * HEAD], ((1,), (0,))).astype(BF16).astype(F32)
    tail = (rim[:, :HEAD] * rim[:, HEAD:])[EXTRA - 8 :]
    for i in range(rows // BLOCK):
        at = pl.ds(i * BLOCK, BLOCK)
        projected = dot(block_rows(x, i), weight[...], ((1,), (0,))).astype(BF16)
        outer = projected[:, :HEAD].astype(F32)
        mixed = projected[:, HEAD : 2 * HEAD].astype(F32) * projected[:, 2 * HEAD : 3 * HEAD].astype(F32)
        one = jnp.where(row == 0, tail[7:8], pltpu.roll(mixed, 1, 0))
        two = jnp.where(row == 0, tail[6:7], jnp.where(row == 1, tail[7:8], pltpu.roll(mixed, 2, 0)))
        conv = tap[0:1] * two + tap[1:2] * one + tap[2:3] * mixed
        tail = mixed[BLOCK - 8 :]
        conv_branch = (outer * conv).astype(BF16)

        query = rotated(projected[:, 3 * HEAD : 4 * HEAD].astype(F32), cosine[at, :], sine[at, :])
        query = query.astype(BF16)
        key, value = keys[at, :], values[at, :]
        here = block_column(column, i)
        line = jnp.concatenate([decay[per * i + j : per * i + j + 1, :] for j in range(per)], axis=1)
        spread = jnp.where(causal, here - line, 0.0)
        scores = jnp.where(causal, dot(query, key, ((1,), (1,))) * jnp.exp(spread), 0.0)
        within = dot(scores.astype(BF16), value, ((1,), (0,)))
        across = dot(query, state.astype(BF16), ((1,), (0,))) * jnp.exp(here - start)
        retained = within + across
        end = line[:, BLOCK - 1 :]
        faded = (key.astype(F32) * jnp.exp(end - here)).astype(BF16)
        state = jnp.exp(end - start) * state + dot(faded, value, ((0,), (0,)))
        start = end
        normed = retained * lax.rsqrt(jnp.mean(retained * retained, axis=-1, keepdims=True) + EPSILON)
        gate = projected[:, 4 * HEAD :].astype(F32)
        ret_branch = (normed * (gate / (1.0 + jnp.exp(-gate)))).astype(BF16)

        half = (i * BLOCK) // (rows // 2)
        place = pl.ds(i * BLOCK - half * (rows // 2), BLOCK)

        @pl.when(own == half)
        def _():
            keep[place, :HEAD] = conv_branch
            keep[place, HEAD:] = ret_branch

        @pl.when(own != half)
        def _():
            send[place, :HEAD] = conv_branch
            send[place, HEAD:] = ret_branch

    copies[1].wait()
    copies[2].wait()


def out_kernel(mine, theirs, weight, out):
    parts, rows = out.shape[0], out.shape[1]
    step = 512
    for column in range(0, out.shape[2], step):
        at = pl.ds(column, step)
        total = dot(mine[...], weight[0, at, :], ((1,), (1,))) + dot(theirs[...], weight[1, at, :], ((1,), (1,)))
        total = total.astype(BF16)
        for part in range(parts):
            out[part, :, column : column + step] = total[part * rows : (part + 1) * rows]


def sum_kernel(parts, out):
    total = parts[0].astype(F32)
    for at in range(1, parts.shape[0]):
        total = total + parts[at].astype(F32)
    out[...] = total.astype(BF16)


def exchanged(x, axes):
    return lax.all_to_all(x, axes, 0, 0, tiled=True)


def body(
    tokens,
    norm_gain,
    conv_outer_weight,
    conv_inner_weight,
    conv_input_weight,
    query_matrix,
    key_weight,
    value_weight,
    gate_weight,
    conv_taps,
    conv_out_weight,
    ret_out_weight,
    log_decay,
):
    own_rows, width = tokens.shape
    tp = lax.axis_size("tp")
    chip = lax.axis_index(CHIPS)
    core = lax.axis_index("core")
    chips = lax.axis_size(CHIPS)
    near, far = lax.axis_size(NEAR), lax.axis_size("za")
    rows = 2 * tp * own_rows
    shard = key_weight.shape[0]

    rest, message = call(
        pack_kernel,
        [slow((shard, 2 * COLUMNS), BF16), fast((2, shard + EXTRA, 2 * HEAD), BF16)],
        "pack",
        specs=[PLAIN] * 10,
        limit=None,
    )(
        key_weight,
        value_weight,
        conv_outer_weight,
        conv_inner_weight,
        conv_input_weight,
        query_matrix,
        gate_weight,
        conv_out_weight.T,
        ret_out_weight.T,
        log_decay.T,
    )
    weights = lax.all_gather(rest, STRETCHES, axis=0, tiled=True)

    own = exchanged(message, "core")
    every_second = lax.all_gather(own.reshape(2 * (shard + EXTRA), 2 * HEAD), FAR)
    pairs = lax.axis_size("zc")
    gathered = exchanged(jnp.broadcast_to(every_second, (pairs, *every_second.shape)), "zc")

    (normed,) = call(norm_kernel, [slow((2 * tp, own_rows, width), BF16)], "norm", specs=[PLAIN] * 2, limit=None)(
        tokens, norm_gain.reshape(1, width)
    )
    x = exchanged(normed, ("core", "tp"))
    halo = lax.ppermute(x[-1, own_rows - EXTRA :], CHIPS, [(i, i + 1) for i in range(chips - 1)])

    inv_freq = ROTARY_BASE ** (-jnp.arange(HALF, dtype=F32) / HALF)
    inv_freq = jnp.concatenate([inv_freq, inv_freq])[None, :]
    far_angle = ((chip * rows).astype(F32) + BLOCK * jnp.arange(8, dtype=F32))[:, None] * inv_freq
    near_angle = jnp.arange(BLOCK, dtype=F32)[:, None] * inv_freq

    keys, values, cosine, sine, decay, column, totals, message = call(
        kv_kernel,
        [
            fast((rows, HEAD), BF16),
            fast((rows, HEAD), BF16),
            fast((rows, HEAD), F32),
            fast((rows, HEAD), F32),
            fast((rows // HEAD, HEAD), F32),
            fast((HEAD, HEAD), F32),
            fast((chips, HEAD), F32),
            fast((near, HEAD, HEAD), BF16),
        ],
        "kv",
        scratch=[pltpu.VMEM((width, 2 * HEAD), BF16)],
        flops=4 * rows * width * HEAD,
    )(x, gathered, own, jnp.cos(far_angle), jnp.sin(far_angle), jnp.cos(near_angle), jnp.sin(near_angle))

    share = HEAD // near
    block = lax.axis_index("za").reshape(1)
    message, before, fade = call(
        near_kernel,
        [fast((far, share, HEAD), BF16), fast((HEAD, HEAD), F32), fast((8, HEAD), F32)],
        "near",
        specs=[SMEM, SMEM, VMEM, VMEM],
        scratch=[pltpu.VMEM((HEAD, HEAD), F32)],
    )(lax.axis_index(NEAR).reshape(1), block, totals, exchanged(message, NEAR))
    (message,) = call(far_kernel, [fast((near, share, HEAD), BF16)], "far", specs=[SMEM, VMEM, VMEM])(
        block, totals, exchanged(message, "za")
    )
    base = exchanged(message, NEAR)

    keep, send, out_weight = call(
        branch_kernel,
        [fast((rows // 2, 2 * HEAD), BF16), fast((rows // 2, 2 * HEAD), BF16), fast((2, width, 2 * HEAD), BF16)],
        "branch",
        specs=[SMEM, ANY] + [VMEM] * 12,
        scratch=[pltpu.VMEM((width, PROJECTED), BF16), pltpu.SemaphoreType.DMA((3,))],
        flops=10 * rows * width * HEAD,
    )(
        core.reshape(1),
        weights,
        x,
        halo,
        cosine,
        sine,
        decay,
        column,
        keys,
        values,
        base,
        before,
        fade,
        conv_taps,
    )
    theirs = lax.ppermute(send, "core", [(0, 1), (1, 0)])
    (partial,) = call(out_kernel, [fast((tp, own_rows, width), BF16)], "out", flops=rows * width * 4 * HEAD)(
        keep, theirs, out_weight
    )
    (mixed,) = call(sum_kernel, [slow((own_rows, width), BF16)], "sum")(exchanged(partial, "tp"))
    return mixed


def solution(mesh):
    groups, stretches, tp = mesh.devices.shape
    chips = stretches // 2
    fine = Mesh(
        mesh.devices.reshape(groups, chips // 4, 2, 2, 2, tp), ("grp", "za", "zb", "zc", "core", "tp")
    )
    columns = P(STRETCHES, "tp")
    placed = (
        P(("grp", *STRETCHES, "tp"), None),
        P(),
        *([columns] * 7),
        P(None, "tp"),
        P("tp", STRETCHES),
        P("tp", STRETCHES),
        P(("grp", *STRETCHES), "tp"),
    )
    return jax.shard_map(
        body, mesh=fine, in_specs=placed, out_specs=P(("grp", *STRETCHES, "tp"), None), check_vma=False
    )
```

```python
import jax
import jax.numpy as jnp
from jax import lax
from jax.experimental import pallas as pl
from jax.experimental.pallas import tpu as pltpu
from jax.sharding import Mesh, PartitionSpec as P

HEAD = 128
HALF = HEAD // 2
CONV_K = 3
EPSILON = 1e-06
ROTARY_BASE = 10000.0
BLOCK = 256
EXTRA = 8
RIM = 16
PROJECTED = 5 * HEAD
INTERPRET = False

BF16 = jnp.bfloat16
F32 = jnp.float32
CHIPS = ("za", "zb", "zc")
STRETCHES = ("za", "zb", "zc", "core")
NEAR = ("zb", "zc")
FAR = ("za", "zb")

VMEM = pl.BlockSpec(memory_space=pltpu.VMEM)
PLAIN = pl.BlockSpec(memory_space=pltpu.VMEM)
SMEM = pl.BlockSpec(memory_space=pltpu.SMEM)
ANY = pl.BlockSpec(memory_space=pl.ANY)


def call(kernel, outs, name, specs=None, scratch=(), flops=0, limit=16):
    def run(*args):
        in_specs = specs if specs is not None else [VMEM] * len(args)
        placed = [placed_for(arg, spec) for arg, spec in zip(args, in_specs)]
        return pl.pallas_call(
            kernel,
            out_shape=[o[0] for o in outs],
            in_specs=in_specs,
            out_specs=[o[1] for o in outs],
            scratch_shapes=list(scratch),
            interpret=INTERPRET,
            name=name,
            compiler_params=pltpu.CompilerParams(vmem_limit_bytes=limit << 20 if limit else None),
            cost_estimate=pl.CostEstimate(flops=flops, bytes_accessed=0, transcendentals=0),
        )(*placed)

    return run


def placed_for(arg, spec):
    if INTERPRET or all(spec is not kind for kind in (VMEM, ANY)):
        return arg
    return pltpu.with_memory_space_constraint(arg, pltpu.VMEM if spec is VMEM else pltpu.HBM)


def fast(dims, kind):
    return (jax.ShapeDtypeStruct(dims, kind) if INTERPRET else pltpu.VMEM(dims, kind), VMEM)


def slow(dims, kind):
    return (jax.ShapeDtypeStruct(dims, kind), VMEM)


def dot(a, b, dims):
    return lax.dot_general(a, b, (dims, ((), ())), preferred_element_type=F32)


def pack_kernel(key, value, conv_out, ret_out, logs, message, outs):
    shard = key.shape[0]
    parts = []
    for core in range(2):
        half = slice(core * HEAD, (core + 1) * HEAD)
        parts += [conv_out[:, half], ret_out[:, half]]
        message[core, :shard, :HEAD] = key[:, half]
        message[core, :shard, HEAD:] = value[:, half]
        lines = [logs[core : core + 1, at : at + 2 * HEAD] for at in range(0, logs.shape[1], 2 * HEAD)]
        line = jnp.concatenate(lines, axis=0)
        high = line.astype(BF16).astype(F32)
        middle = (line - high).astype(BF16).astype(F32)
        low = line - high - middle
        filler = jnp.zeros((EXTRA - 3 * len(lines), 2 * HEAD), F32)
        message[core, shard:, :] = jnp.concatenate([high, middle, low, filler], axis=0).astype(BF16)
    both = jnp.concatenate(parts, axis=1)
    for copy in range(outs.shape[0]):
        outs[copy] = both


def join_kernel(*refs):
    *inputs, outs, rest = refs
    for at, ref in enumerate(inputs):
        for core in range(2):
            to = core * PROJECTED + at * HEAD
            rest[:, to : to + HEAD] = ref[:, core * HEAD : (core + 1) * HEAD]
    each = outs.shape[2]
    for part in range(outs.shape[0]):
        to = 2 * PROJECTED + part * each
        rest[:, to : to + each] = outs[part]


def logs_of(rows, lines):
    rows = rows.astype(F32)
    return rows[:lines] + rows[lines : 2 * lines] + rows[2 * lines : 3 * lines]


def norm_kernel(tokens, gain, out):
    values = tokens[...].astype(F32)
    scale = lax.rsqrt(jnp.mean(values * values, axis=-1, keepdims=True) + EPSILON)
    normed = (values * scale * gain[...].astype(F32)[None, :]).astype(BF16)
    for copy in range(out.shape[0]):
        out[copy] = normed


def rotated(head, cosine, sine):
    return head * cosine + pltpu.roll(head, HALF, 1) * sine


def kv_kernel(
    pair, x, same, other, own, cos_far, sin_far, cos_near, sin_near, k_out, v_out, cosine, sine, decay, column, totals, message, weight
):
    rows, width = x.shape[0] * x.shape[1], x.shape[2]
    fars = same.shape[0]
    shard = own.shape[1] - EXTRA
    lines = rows // 2 // (2 * HEAD)

    pieces = []
    for core in range(2):
        logs = logs_of(own[core, shard:, :], lines)
        for line in range(lines):
            pieces += [logs[line : line + 1, :HEAD], logs[line : line + 1, HEAD:]]
    logs = jnp.concatenate(pieces, axis=0)
    upper = lax.broadcasted_iota(jnp.int32, (HEAD, HEAD), 0) <= lax.broadcasted_iota(jnp.int32, (HEAD, HEAD), 1)
    inner = lax.dot_general(
        logs,
        upper.astype(F32),
        (((1,), (0,)), ((), ())),
        precision=lax.Precision.HIGHEST,
        preferred_element_type=F32,
    )
    before = jnp.zeros((1, 1), F32)
    added = []
    for at in range(len(pieces)):
        added.append(inner[at : at + 1] + before)
        before = before + inner[at : at + 1, HEAD - 1 :]
    cumulative = jnp.concatenate(added, axis=0)
    decay[...] = cumulative
    filler = jnp.zeros((HEAD - len(pieces), HEAD), F32)
    column[...] = jnp.concatenate([cumulative, filler], axis=0).T
    total = before

    for source, place in ((same, pair[0]), (other, 1 - pair[0])):
        for far in range(fars):
            chip = 2 * far + place
            log_total = jnp.zeros((1, 1), F32)
            for core in range(2):
                at = core * (shard + EXTRA)
                to = pl.multiple_of((2 * chip + core) * shard, shard)
                weight[pl.ds(to, shard), :] = source[far, at : at + shard, :]
                logs = logs_of(source[far, at + shard : at + shard + EXTRA, :], lines)
                log_total = log_total + jnp.sum(logs, axis=(0, 1), keepdims=True)
            totals[pl.ds(chip, 1), :] = jnp.broadcast_to(log_total, (1, HEAD))

    state = jnp.zeros((HEAD, HEAD), F32)
    for i in range(rows // BLOCK):
        at = pl.ds(i * BLOCK, BLOCK)
        cos_at = cos_far[i : i + 1, :] * cos_near[...] - sin_far[i : i + 1, :] * sin_near[...]
        sin_at = sin_far[i : i + 1, :] * cos_near[...] + cos_far[i : i + 1, :] * sin_near[...]
        first = lax.broadcasted_iota(jnp.int32, sin_at.shape, 1) < HALF
        sin_at = jnp.where(first, -sin_at, sin_at)
        cosine[at, :] = cos_at
        sine[at, :] = sin_at
        both = dot(block_rows(x, i), weight[...], ((1,), (0,))).astype(BF16)
        key = rotated(both[:, :HEAD].astype(F32), cos_at, sin_at) * HEAD ** (-0.5)
        k_out[at, :] = key.astype(BF16)
        value = both[:, HEAD:]
        v_out[at, :] = value
        here = block_column(column, i)
        faded = (key * jnp.exp(total - here)).astype(BF16)
        state = state + dot(faded, value, ((0,), (0,)))
    for copy in range(message.shape[0]):
        message[copy] = state.astype(BF16)


def block_rows(x, i):
    per = BLOCK // x.shape[1]
    return x[i * per : (i + 1) * per].reshape(BLOCK, x.shape[2])


def block_column(column, i):
    per = BLOCK // HEAD
    return jnp.concatenate([column[:, per * i + j : per * i + j + 1] for j in range(per)], axis=0)


def near_kernel(place, block, totals, gathered, message, before, fade, scratch):
    own = place[0]
    near = gathered.shape[0]
    run = jnp.zeros((HEAD, HEAD), F32)
    passed = jnp.zeros((1, HEAD), F32)
    kept, kept_passed = run, passed
    for at in range(near):
        kept = jnp.where(own == at, run, kept)
        kept_passed = jnp.where(own == at, passed, kept_passed)
        log_total = totals[pl.ds(block[0] * near + at, 1), :]
        run = jnp.exp(log_total) * run + gathered[at].astype(F32)
        passed = passed + log_total
    before[...] = kept
    fade[...] = jnp.broadcast_to(jnp.exp(kept_passed), fade.shape)
    scratch[...] = run
    share = HEAD // near
    part = scratch[pl.ds(pl.multiple_of(own * share, share), share), :].astype(BF16)
    for copy in range(message.shape[0]):
        message[copy] = part


def far_kernel(place, totals, gathered, message):
    own = place[0]
    near, share = message.shape[:2]
    run = jnp.zeros((share, HEAD), F32)
    kept = run
    for at in range(gathered.shape[0]):
        kept = jnp.where(own == at, run, kept)
        log_total = jnp.sum(totals[at * near : (at + 1) * near, :], axis=0, keepdims=True)
        run = jnp.exp(log_total) * run + gathered[at].astype(F32)
    for copy in range(near):
        message[copy] = kept.astype(BF16)


def branch_kernel(
    core,
    weights,
    x,
    halo,
    cosine,
    sine,
    decay,
    column,
    keys,
    values,
    base,
    before,
    fade,
    taps,
    branches,
    out_weight,
    weight,
    semaphores,
):
    rows = x.shape[0] * x.shape[1]
    own = core[0]
    start_at = pl.multiple_of(own * PROJECTED, HEAD)
    copies = [
        pltpu.make_async_copy(weights.at[:, pl.ds(start_at, PROJECTED)], weight, semaphores.at[0]),
        pltpu.make_async_copy(
            weights.at[:, pl.ds(2 * PROJECTED, out_weight.shape[1])], out_weight, semaphores.at[1]
        ),
    ]
    for copy in copies:
        copy.start()
    incoming = jnp.concatenate([base[at].astype(F32) for at in range(base.shape[0])], axis=0)
    state = fade[0:1, :] * incoming + before[...]
    row = lax.broadcasted_iota(jnp.int32, (BLOCK, HEAD), 0)
    causal = lax.broadcasted_iota(jnp.int32, (BLOCK, BLOCK), 0) >= lax.broadcasted_iota(
        jnp.int32, (BLOCK, BLOCK), 1
    )
    tap = jnp.where(own == 0, taps[:, :HEAD].astype(F32), taps[:, HEAD:].astype(F32))
    start = jnp.zeros((1, 1), F32)
    per = BLOCK // HEAD
    copies[0].wait()
    rim = dot(halo[...], weight[:, HEAD : 3 * HEAD], ((1,), (0,))).astype(BF16).astype(F32)
    tail = (rim[:, :HEAD] * rim[:, HEAD:])[RIM - 8 :]
    for i in range(rows // BLOCK):
        at = pl.ds(i * BLOCK, BLOCK)
        projected = dot(block_rows(x, i), weight[...], ((1,), (0,))).astype(BF16)
        outer = projected[:, :HEAD].astype(F32)
        mixed = projected[:, HEAD : 2 * HEAD].astype(F32) * projected[:, 2 * HEAD : 3 * HEAD].astype(F32)
        one = jnp.where(row == 0, tail[7:8], pltpu.roll(mixed, 1, 0))
        two = jnp.where(row == 0, tail[6:7], jnp.where(row == 1, tail[7:8], pltpu.roll(mixed, 2, 0)))
        conv = tap[0:1] * two + tap[1:2] * one + tap[2:3] * mixed
        tail = mixed[BLOCK - 8 :]
        conv_branch = (outer * conv).astype(BF16)

        query = rotated(projected[:, 3 * HEAD : 4 * HEAD].astype(F32), cosine[at, :], sine[at, :])
        query = query.astype(BF16)
        key, value = keys[at, :], values[at, :]
        here = block_column(column, i)
        line = jnp.concatenate([decay[per * i + j : per * i + j + 1, :] for j in range(per)], axis=1)
        spread = jnp.where(causal, here - line, 0.0)
        scores = jnp.where(causal, dot(query, key, ((1,), (1,))) * jnp.exp(spread), 0.0)
        within = dot(scores.astype(BF16), value, ((1,), (0,)))
        across = dot(query, state.astype(BF16), ((1,), (0,))) * jnp.exp(here - start)
        retained = within + across
        end = line[:, BLOCK - 1 :]
        faded = (key.astype(F32) * jnp.exp(end - here)).astype(BF16)
        state = jnp.exp(end - start) * state + dot(faded, value, ((0,), (0,)))
        start = end
        normed = retained * lax.rsqrt(jnp.mean(retained * retained, axis=-1, keepdims=True) + EPSILON)
        gate = projected[:, 4 * HEAD :].astype(F32)
        ret_branch = (normed * (gate / (1.0 + jnp.exp(-gate)))).astype(BF16)

        per_part = branches.shape[1]
        for part in range(BLOCK // per_part):
            rows_at = slice(part * per_part, (part + 1) * per_part)
            branches[i * BLOCK // per_part + part, :, :HEAD] = conv_branch[rows_at]
            branches[i * BLOCK // per_part + part, :, HEAD:] = ret_branch[rows_at]

    copies[1].wait()


def out_kernel(branches, weight, out):
    parts = branches.shape[0] // 2
    order = [branches[core * parts + part] for part in range(parts) for core in range(2)]
    rows = jnp.concatenate(order, axis=1)
    step = 512
    for column in range(0, out.shape[1], step):
        out[:, column : column + step] = dot(rows, weight[column : column + step, :], ((1,), (1,))).astype(BF16)


def exchanged(x, axes):
    return lax.all_to_all(x, axes, 0, 0, tiled=True)


def body(
    tokens,
    norm_gain,
    conv_outer_weight,
    conv_inner_weight,
    conv_input_weight,
    query_matrix,
    key_weight,
    value_weight,
    gate_weight,
    conv_taps,
    conv_out_weight,
    ret_out_weight,
    log_decay,
):
    own_rows, width = tokens.shape
    tp = lax.axis_size("tp")
    chip = lax.axis_index(CHIPS)
    core = lax.axis_index("core")
    chips = lax.axis_size(CHIPS)
    near, far = lax.axis_size(NEAR), lax.axis_size("za")
    rows = 2 * tp * own_rows
    shard = key_weight.shape[0]

    message, outs = call(
        pack_kernel,
        [fast((2, shard + EXTRA, 2 * HEAD), BF16), fast((tp, shard, 4 * HEAD), BF16)],
        "pack",
        specs=[PLAIN] * 5,
        limit=None,
    )(key_weight, value_weight, conv_out_weight.T, ret_out_weight.T, log_decay.T)
    inputs = (conv_outer_weight, conv_inner_weight, conv_input_weight, query_matrix, gate_weight)
    (rest,) = call(
        join_kernel, [slow((shard, 2 * PROJECTED + 4 * HEAD * tp), BF16)], "join", specs=[PLAIN] * 6, limit=None
    )(*inputs, exchanged(outs, "tp"))
    weights = lax.all_gather(rest, STRETCHES, axis=0, tiled=True)

    own = exchanged(message, "core")
    same = lax.all_gather(own.reshape(2 * (shard + EXTRA), 2 * HEAD), FAR)
    other = lax.ppermute(same, "zc", [(0, 1), (1, 0)])

    (normed,) = call(norm_kernel, [slow((2 * tp, own_rows, width), BF16)], "norm", specs=[PLAIN] * 2, limit=None)(
        tokens, norm_gain
    )
    x = exchanged(normed, ("core", "tp"))
    halo = lax.ppermute(x[-1, own_rows - RIM :], CHIPS, [(i, i + 1) for i in range(chips - 1)])

    inv_freq = ROTARY_BASE ** (-jnp.arange(HALF, dtype=F32) / HALF)
    inv_freq = jnp.concatenate([inv_freq, inv_freq])[None, :]
    far_angle = ((chip * rows).astype(F32) + BLOCK * jnp.arange(8, dtype=F32))[:, None] * inv_freq
    near_angle = jnp.arange(BLOCK, dtype=F32)[:, None] * inv_freq

    keys, values, cosine, sine, decay, column, totals, message = call(
        kv_kernel,
        [
            fast((rows, HEAD), BF16),
            fast((rows, HEAD), BF16),
            fast((rows, HEAD), F32),
            fast((rows, HEAD), F32),
            fast((rows // HEAD, HEAD), F32),
            fast((HEAD, HEAD), F32),
            fast((chips, HEAD), F32),
            fast((near, HEAD, HEAD), BF16),
        ],
        "kv",
        specs=[SMEM] + [VMEM] * 8,
        scratch=[pltpu.VMEM((width, 2 * HEAD), BF16)],
        flops=4 * rows * width * HEAD,
    )(lax.axis_index("zc").reshape(1), x, same, other, own, jnp.cos(far_angle), jnp.sin(far_angle), jnp.cos(near_angle), jnp.sin(near_angle))

    share = HEAD // near
    block = lax.axis_index("za").reshape(1)
    message, before, fade = call(
        near_kernel,
        [fast((far, share, HEAD), BF16), fast((HEAD, HEAD), F32), fast((8, HEAD), F32)],
        "near",
        specs=[SMEM, SMEM, VMEM, VMEM],
        scratch=[pltpu.VMEM((HEAD, HEAD), F32)],
    )(lax.axis_index(NEAR).reshape(1), block, totals, exchanged(message, NEAR))
    (message,) = call(far_kernel, [fast((near, share, HEAD), BF16)], "far", specs=[SMEM, VMEM, VMEM])(
        block, totals, exchanged(message, "za")
    )
    base = exchanged(message, NEAR)

    parts = 2 * tp
    branches, out_weight = call(
        branch_kernel,
        [fast((parts, own_rows, 2 * HEAD), BF16), fast((width, 2 * HEAD * parts), BF16)],
        "branch",
        specs=[SMEM, ANY] + [VMEM] * 12,
        scratch=[pltpu.VMEM((width, PROJECTED), BF16), pltpu.SemaphoreType.DMA((2,))],
        flops=10 * rows * width * HEAD,
    )(
        core.reshape(1),
        weights,
        x,
        halo,
        cosine,
        sine,
        decay,
        column,
        keys,
        values,
        base,
        before,
        fade,
        conv_taps,
    )
    (mixed,) = call(out_kernel, [slow((own_rows, width), BF16)], "out", flops=rows * width * 4 * HEAD)(
        exchanged(branches, ("core", "tp")), out_weight
    )
    return mixed


def solution(mesh):
    groups, stretches, tp = mesh.devices.shape
    chips = stretches // 2
    fine = Mesh(
        mesh.devices.reshape(groups, chips // 4, 2, 2, 2, tp), ("grp", "za", "zb", "zc", "core", "tp")
    )
    columns = P(STRETCHES, "tp")
    placed = (
        P(("grp", *STRETCHES, "tp"), None),
        P(),
        *([columns] * 7),
        P(None, "tp"),
        P("tp", STRETCHES),
        P("tp", STRETCHES),
        P(("grp", *STRETCHES), "tp"),
    )
    return jax.shard_map(
        body, mesh=fine, in_specs=placed, out_specs=P(("grp", *STRETCHES, "tp"), None), check_vma=False
    )
```

```python
import jax
import jax.numpy as jnp
from jax import lax
from jax.experimental import pallas as pl
from jax.experimental.pallas import tpu as pltpu
from jax.sharding import Mesh, PartitionSpec as P

HEAD = 128
HALF = HEAD // 2
CONV_K = 3
EPSILON = 1e-06
ROTARY_BASE = 10000.0
BLOCK = 256
EXTRA = 8
RIM = 16
PROJECTED = 5 * HEAD
COLUMNS = 7 * HEAD
INTERPRET = False

BF16 = jnp.bfloat16
F32 = jnp.float32
CHIPS = ("za", "zb", "zc")
STRETCHES = ("za", "zb", "zc", "core")
NEAR = ("zb", "zc")
FAR = ("za", "zb")

VMEM = pl.BlockSpec(memory_space=pltpu.VMEM)
PLAIN = pl.BlockSpec(memory_space=pltpu.VMEM)
SMEM = pl.BlockSpec(memory_space=pltpu.SMEM)
ANY = pl.BlockSpec(memory_space=pl.ANY)


def call(kernel, outs, name, specs=None, scratch=(), flops=0, limit=16):
    def run(*args):
        in_specs = specs if specs is not None else [VMEM] * len(args)
        placed = [placed_for(arg, spec) for arg, spec in zip(args, in_specs)]
        return pl.pallas_call(
            kernel,
            out_shape=[o[0] for o in outs],
            in_specs=in_specs,
            out_specs=[o[1] for o in outs],
            scratch_shapes=list(scratch),
            interpret=INTERPRET,
            name=name,
            compiler_params=pltpu.CompilerParams(vmem_limit_bytes=limit << 20 if limit else None),
            cost_estimate=pl.CostEstimate(flops=flops, bytes_accessed=0, transcendentals=0),
        )(*placed)

    return run


def placed_for(arg, spec):
    if INTERPRET or all(spec is not kind for kind in (VMEM, ANY)):
        return arg
    return pltpu.with_memory_space_constraint(arg, pltpu.VMEM if spec is VMEM else pltpu.HBM)


def fast(dims, kind):
    return (jax.ShapeDtypeStruct(dims, kind) if INTERPRET else pltpu.VMEM(dims, kind), VMEM)


def slow(dims, kind):
    return (jax.ShapeDtypeStruct(dims, kind), VMEM)


def dot(a, b, dims):
    return lax.dot_general(a, b, (dims, ((), ())), preferred_element_type=F32)


def pack_kernel(key, value, *refs):
    *inputs, logs, rest, message = refs
    for at, ref in enumerate(inputs):
        for core in range(2):
            to = core * COLUMNS + at * HEAD
            rest[:, to : to + HEAD] = ref[:, core * HEAD : (core + 1) * HEAD]
    shard = key.shape[0]
    for core in range(2):
        message[core, :shard, :HEAD] = key[:, core * HEAD : (core + 1) * HEAD]
        message[core, :shard, HEAD:] = value[:, core * HEAD : (core + 1) * HEAD]
        lines = [logs[core : core + 1, at : at + 2 * HEAD] for at in range(0, logs.shape[1], 2 * HEAD)]
        line = jnp.concatenate(lines, axis=0)
        high = line.astype(BF16).astype(F32)
        middle = (line - high).astype(BF16).astype(F32)
        low = line - high - middle
        filler = jnp.zeros((EXTRA - 3 * len(lines), 2 * HEAD), F32)
        message[core, shard:, :] = jnp.concatenate([high, middle, low, filler], axis=0).astype(BF16)


def logs_of(rows, lines):
    rows = rows.astype(F32)
    return rows[:lines] + rows[lines : 2 * lines] + rows[2 * lines : 3 * lines]


def norm_kernel(tokens, gain, out):
    values = tokens[...].astype(F32)
    scale = lax.rsqrt(jnp.mean(values * values, axis=-1, keepdims=True) + EPSILON)
    normed = (values * scale * gain[...].astype(F32)[None, :]).astype(BF16)
    for copy in range(out.shape[0]):
        out[copy] = normed


def rotated(head, cosine, sine):
    return head * cosine + pltpu.roll(head, HALF, 1) * sine


def kv_kernel(
    pair, x, same, low, high, own, cos_far, sin_far, cos_near, sin_near, k_out, v_out, cosine, sine, decay, column, totals, message, weight
):
    rows, width = x.shape[0] * x.shape[1], x.shape[2]
    half = low.shape[0]
    shard = own.shape[1] - EXTRA
    lines = rows // 2 // (2 * HEAD)

    pieces = []
    for core in range(2):
        logs = logs_of(own[core, shard:, :], lines)
        for line in range(lines):
            pieces += [logs[line : line + 1, :HEAD], logs[line : line + 1, HEAD:]]
    logs = jnp.concatenate(pieces, axis=0)
    upper = lax.broadcasted_iota(jnp.int32, (HEAD, HEAD), 0) <= lax.broadcasted_iota(jnp.int32, (HEAD, HEAD), 1)
    inner = lax.dot_general(
        logs,
        upper.astype(F32),
        (((1,), (0,)), ((), ())),
        precision=lax.Precision.HIGHEST,
        preferred_element_type=F32,
    )
    before = jnp.zeros((1, 1), F32)
    added = []
    for at in range(len(pieces)):
        added.append(inner[at : at + 1] + before)
        before = before + inner[at : at + 1, HEAD - 1 :]
    cumulative = jnp.concatenate(added, axis=0)
    decay[...] = cumulative
    filler = jnp.zeros((HEAD - len(pieces), HEAD), F32)
    column[...] = jnp.concatenate([cumulative, filler], axis=0).T
    total = before

    mine, others = pair[0], 1 - pair[0]
    for source, first, place in ((same, 0, mine), (low, 0, others), (high, half, others)):
        for at_far in range(source.shape[0]):
            chip = 2 * (first + at_far) + place
            log_total = jnp.zeros((1, 1), F32)
            for core in range(2):
                at = core * (shard + EXTRA)
                to = pl.multiple_of((2 * chip + core) * shard, shard)
                weight[pl.ds(to, shard), :] = source[at_far, at : at + shard, :]
                logs = logs_of(source[at_far, at + shard : at + shard + EXTRA, :], lines)
                log_total = log_total + jnp.sum(logs, axis=(0, 1), keepdims=True)
            totals[pl.ds(chip, 1), :] = jnp.broadcast_to(log_total, (1, HEAD))

    state = jnp.zeros((HEAD, HEAD), F32)
    for i in range(rows // BLOCK):
        at = pl.ds(i * BLOCK, BLOCK)
        cos_at = cos_far[i : i + 1, :] * cos_near[...] - sin_far[i : i + 1, :] * sin_near[...]
        sin_at = sin_far[i : i + 1, :] * cos_near[...] + cos_far[i : i + 1, :] * sin_near[...]
        first = lax.broadcasted_iota(jnp.int32, sin_at.shape, 1) < HALF
        sin_at = jnp.where(first, -sin_at, sin_at)
        cosine[at, :] = cos_at
        sine[at, :] = sin_at
        both = dot(block_rows(x, i), weight[...], ((1,), (0,))).astype(BF16)
        key = rotated(both[:, :HEAD].astype(F32), cos_at, sin_at) * HEAD ** (-0.5)
        k_out[at, :] = key.astype(BF16)
        value = both[:, HEAD:]
        v_out[at, :] = value
        here = block_column(column, i)
        faded = (key * jnp.exp(total - here)).astype(BF16)
        state = state + dot(faded, value, ((0,), (0,)))
    for copy in range(message.shape[0]):
        message[copy] = state.astype(BF16)


def block_rows(x, i):
    per = BLOCK // x.shape[1]
    return x[i * per : (i + 1) * per].reshape(BLOCK, x.shape[2])


def block_column(column, i):
    per = BLOCK // HEAD
    return jnp.concatenate([column[:, per * i + j : per * i + j + 1] for j in range(per)], axis=0)


def near_kernel(place, block, totals, gathered, message, before, fade, scratch):
    own = place[0]
    near = gathered.shape[0]
    run = jnp.zeros((HEAD, HEAD), F32)
    passed = jnp.zeros((1, HEAD), F32)
    kept, kept_passed = run, passed
    for at in range(near):
        kept = jnp.where(own == at, run, kept)
        kept_passed = jnp.where(own == at, passed, kept_passed)
        log_total = totals[pl.ds(block[0] * near + at, 1), :]
        run = jnp.exp(log_total) * run + gathered[at].astype(F32)
        passed = passed + log_total
    before[...] = kept
    fade[...] = jnp.broadcast_to(jnp.exp(kept_passed), fade.shape)
    scratch[...] = run
    share = HEAD // near
    part = scratch[pl.ds(pl.multiple_of(own * share, share), share), :].astype(BF16)
    for copy in range(message.shape[0]):
        message[copy] = part


def far_kernel(place, totals, gathered, message):
    own = place[0]
    near, share = message.shape[:2]
    run = jnp.zeros((share, HEAD), F32)
    kept = run
    for at in range(gathered.shape[0]):
        kept = jnp.where(own == at, run, kept)
        log_total = jnp.sum(totals[at * near : (at + 1) * near, :], axis=0, keepdims=True)
        run = jnp.exp(log_total) * run + gathered[at].astype(F32)
    for copy in range(near):
        message[copy] = kept.astype(BF16)


def store(own, i, rows, keep, send, channel, branch):
    half = (i * BLOCK) // (rows // 2)
    place = slice(i * BLOCK - half * (rows // 2), (i + 1) * BLOCK - half * (rows // 2))

    @pl.when(own == half)
    def _():
        keep[place, channel : channel + HEAD] = branch

    @pl.when(own != half)
    def _():
        send[place, channel : channel + HEAD] = branch


def branch_kernel(
    core,
    weights,
    x,
    halo,
    cosine,
    sine,
    decay,
    column,
    keys,
    values,
    base,
    before,
    fade,
    taps,
    keep,
    send,
    out_weight,
    conv_weight,
    ret_weight,
    semaphores,
):
    rows = x.shape[0] * x.shape[1]
    own = core[0]
    start_at = pl.multiple_of(own * COLUMNS, HEAD)
    other_at = pl.multiple_of((1 - own) * COLUMNS, HEAD)
    copies = [
        pltpu.make_async_copy(weights.at[:, pl.ds(start_at, 3 * HEAD)], conv_weight, semaphores.at[0]),
        pltpu.make_async_copy(
            weights.at[:, pl.ds(start_at + 3 * HEAD, 2 * HEAD)], ret_weight, semaphores.at[1]
        ),
        pltpu.make_async_copy(
            weights.at[:, pl.ds(start_at + PROJECTED, 2 * HEAD)], out_weight.at[0], semaphores.at[2]
        ),
        pltpu.make_async_copy(
            weights.at[:, pl.ds(other_at + PROJECTED, 2 * HEAD)], out_weight.at[1], semaphores.at[3]
        ),
    ]
    for copy in copies:
        copy.start()
    incoming = jnp.concatenate([base[at].astype(F32) for at in range(base.shape[0])], axis=0)
    state = fade[0:1, :] * incoming + before[...]
    row = lax.broadcasted_iota(jnp.int32, (BLOCK, HEAD), 0)
    causal = lax.broadcasted_iota(jnp.int32, (BLOCK, BLOCK), 0) >= lax.broadcasted_iota(
        jnp.int32, (BLOCK, BLOCK), 1
    )
    tap = jnp.where(own == 0, taps[:, :HEAD].astype(F32), taps[:, HEAD:].astype(F32))
    start = jnp.zeros((1, 1), F32)
    per = BLOCK // HEAD
    copies[0].wait()
    rim = dot(halo[...], conv_weight[:, HEAD:], ((1,), (0,))).astype(BF16).astype(F32)
    tail = (rim[:, :HEAD] * rim[:, HEAD:])[RIM - 8 :]
    for i in range(rows // BLOCK):
        projected = dot(block_rows(x, i), conv_weight[...], ((1,), (0,))).astype(BF16)
        outer = projected[:, :HEAD].astype(F32)
        mixed = projected[:, HEAD : 2 * HEAD].astype(F32) * projected[:, 2 * HEAD :].astype(F32)
        one = jnp.where(row == 0, tail[7:8], pltpu.roll(mixed, 1, 0))
        two = jnp.where(row == 0, tail[6:7], jnp.where(row == 1, tail[7:8], pltpu.roll(mixed, 2, 0)))
        conv = tap[0:1] * two + tap[1:2] * one + tap[2:3] * mixed
        tail = mixed[BLOCK - 8 :]
        store(own, i, rows, keep, send, 0, (outer * conv).astype(BF16))

    copies[1].wait()
    for i in range(rows // BLOCK):
        at = pl.ds(i * BLOCK, BLOCK)
        projected = dot(block_rows(x, i), ret_weight[...], ((1,), (0,))).astype(BF16)
        query = rotated(projected[:, :HEAD].astype(F32), cosine[at, :], sine[at, :])
        query = query.astype(BF16)
        key, value = keys[at, :], values[at, :]
        here = block_column(column, i)
        line = jnp.concatenate([decay[per * i + j : per * i + j + 1, :] for j in range(per)], axis=1)
        spread = jnp.where(causal, here - line, 0.0)
        scores = jnp.where(causal, dot(query, key, ((1,), (1,))) * jnp.exp(spread), 0.0)
        within = dot(scores.astype(BF16), value, ((1,), (0,)))
        across = dot(query, state.astype(BF16), ((1,), (0,))) * jnp.exp(here - start)
        retained = within + across
        end = line[:, BLOCK - 1 :]
        faded = (key.astype(F32) * jnp.exp(end - here)).astype(BF16)
        state = jnp.exp(end - start) * state + dot(faded, value, ((0,), (0,)))
        start = end
        normed = retained * lax.rsqrt(jnp.mean(retained * retained, axis=-1, keepdims=True) + EPSILON)
        gate = projected[:, HEAD:].astype(F32)
        ret_branch = (normed * (gate / (1.0 + jnp.exp(-gate)))).astype(BF16)

        store(own, i, rows, keep, send, HEAD, ret_branch)

    copies[2].wait()
    copies[3].wait()


def out_kernel(mine, theirs, weight, out):
    parts, rows = out.shape[0], out.shape[1]
    step = 512
    for column in range(0, out.shape[2], step):
        at = pl.ds(column, step)
        total = dot(mine[...], weight[0, at, :], ((1,), (1,))) + dot(theirs[...], weight[1, at, :], ((1,), (1,)))
        total = total.astype(BF16)
        for part in range(parts):
            out[part, :, column : column + step] = total[part * rows : (part + 1) * rows]


def sum_kernel(parts, out):
    total = parts[0].astype(F32)
    for at in range(1, parts.shape[0]):
        total = total + parts[at].astype(F32)
    out[...] = total.astype(BF16)


def exchanged(x, axes):
    return lax.all_to_all(x, axes, 0, 0, tiled=True)


def body(
    tokens,
    norm_gain,
    conv_outer_weight,
    conv_inner_weight,
    conv_input_weight,
    query_matrix,
    key_weight,
    value_weight,
    gate_weight,
    conv_taps,
    conv_out_weight,
    ret_out_weight,
    log_decay,
):
    own_rows, width = tokens.shape
    tp = lax.axis_size("tp")
    chip = lax.axis_index(CHIPS)
    core = lax.axis_index("core")
    chips = lax.axis_size(CHIPS)
    near, far = lax.axis_size(NEAR), lax.axis_size("za")
    rows = 2 * tp * own_rows
    shard = key_weight.shape[0]

    rest, message = call(
        pack_kernel,
        [slow((shard, 2 * COLUMNS), BF16), fast((2, shard + EXTRA, 2 * HEAD), BF16)],
        "pack",
        specs=[PLAIN] * 10,
        limit=None,
    )(
        key_weight,
        value_weight,
        conv_outer_weight,
        conv_inner_weight,
        conv_input_weight,
        query_matrix,
        gate_weight,
        conv_out_weight.T,
        ret_out_weight.T,
        log_decay.T,
    )
    weights = lax.all_gather(rest, STRETCHES, axis=0, tiled=True)

    own = exchanged(message, "core")
    same = lax.all_gather(own.reshape(2 * (shard + EXTRA), 2 * HEAD), FAR)
    half = same.shape[0] // 2
    low = lax.ppermute(same[:half], CHIPS, [(i, (i - 1) % chips) for i in range(chips)])
    high = lax.ppermute(same[half:], CHIPS, [(i, (i + 1) % chips) for i in range(chips)])

    (normed,) = call(norm_kernel, [slow((2 * tp, own_rows, width), BF16)], "norm", specs=[PLAIN] * 2, limit=None)(
        tokens, norm_gain
    )
    x = exchanged(normed, ("core", "tp"))
    halo = lax.ppermute(x[-1, own_rows - RIM :], CHIPS, [(i, i + 1) for i in range(chips - 1)])

    inv_freq = ROTARY_BASE ** (-jnp.arange(HALF, dtype=F32) / HALF)
    inv_freq = jnp.concatenate([inv_freq, inv_freq])[None, :]
    far_angle = ((chip * rows).astype(F32) + BLOCK * jnp.arange(8, dtype=F32))[:, None] * inv_freq
    near_angle = jnp.arange(BLOCK, dtype=F32)[:, None] * inv_freq

    keys, values, cosine, sine, decay, column, totals, message = call(
        kv_kernel,
        [
            fast((rows, HEAD), BF16),
            fast((rows, HEAD), BF16),
            fast((rows, HEAD), F32),
            fast((rows, HEAD), F32),
            fast((rows // HEAD, HEAD), F32),
            fast((HEAD, HEAD), F32),
            fast((chips, HEAD), F32),
            fast((near, HEAD, HEAD), BF16),
        ],
        "kv",
        specs=[SMEM] + [VMEM] * 9,
        scratch=[pltpu.VMEM((width, 2 * HEAD), BF16)],
        flops=4 * rows * width * HEAD,
    )(lax.axis_index("zc").reshape(1), x, same, low, high, own, jnp.cos(far_angle), jnp.sin(far_angle), jnp.cos(near_angle), jnp.sin(near_angle))

    share = HEAD // near
    block = lax.axis_index("za").reshape(1)
    message, before, fade = call(
        near_kernel,
        [fast((far, share, HEAD), BF16), fast((HEAD, HEAD), F32), fast((8, HEAD), F32)],
        "near",
        specs=[SMEM, SMEM, VMEM, VMEM],
        scratch=[pltpu.VMEM((HEAD, HEAD), F32)],
    )(lax.axis_index(NEAR).reshape(1), block, totals, exchanged(message, NEAR))
    (message,) = call(far_kernel, [fast((near, share, HEAD), BF16)], "far", specs=[SMEM, VMEM, VMEM])(
        block, totals, exchanged(message, "za")
    )
    base = exchanged(message, NEAR)

    keep, send, out_weight = call(
        branch_kernel,
        [fast((rows // 2, 2 * HEAD), BF16), fast((rows // 2, 2 * HEAD), BF16), fast((2, width, 2 * HEAD), BF16)],
        "branch",
        specs=[SMEM, ANY] + [VMEM] * 12,
        scratch=[
            pltpu.VMEM((width, 3 * HEAD), BF16),
            pltpu.VMEM((width, 2 * HEAD), BF16),
            pltpu.SemaphoreType.DMA((4,)),
        ],
        flops=10 * rows * width * HEAD,
    )(
        core.reshape(1),
        weights,
        x,
        halo,
        cosine,
        sine,
        decay,
        column,
        keys,
        values,
        base,
        before,
        fade,
        conv_taps,
    )
    theirs = lax.ppermute(send, "core", [(0, 1), (1, 0)])
    (partial,) = call(out_kernel, [fast((tp, own_rows, width), BF16)], "out", flops=rows * width * 4 * HEAD)(
        keep, theirs, out_weight
    )
    (mixed,) = call(sum_kernel, [slow((own_rows, width), BF16)], "sum")(exchanged(partial, "tp"))
    return mixed


def solution(mesh):
    groups, stretches, tp = mesh.devices.shape
    chips = stretches // 2
    fine = Mesh(
        mesh.devices.reshape(groups, chips // 4, 2, 2, 2, tp), ("grp", "za", "zb", "zc", "core", "tp")
    )
    columns = P(STRETCHES, "tp")
    placed = (
        P(("grp", *STRETCHES, "tp"), None),
        P(),
        *([columns] * 7),
        P(None, "tp"),
        P("tp", STRETCHES),
        P("tp", STRETCHES),
        P(("grp", *STRETCHES), "tp"),
    )
    return jax.shard_map(
        body, mesh=fine, in_specs=placed, out_specs=P(("grp", *STRETCHES, "tp"), None), check_vma=False
    )
```

```python
import jax
import jax.numpy as jnp
from jax import lax
from jax.experimental import pallas as pl
from jax.experimental.pallas import tpu as pltpu
from jax.sharding import Mesh, PartitionSpec as P

HEAD = 128
HALF = HEAD // 2
CONV_K = 3
EPSILON = 1e-06
ROTARY_BASE = 10000.0
BLOCK = 256
EXTRA = 8
RIM = 16
PROJECTED = 5 * HEAD
PIECES = 4
COLUMNS = 7 * HEAD
INTERPRET = False

BF16 = jnp.bfloat16
F32 = jnp.float32
CHIPS = ("za", "zb", "zc")
STRETCHES = ("za", "zb", "zc", "core")
NEAR = ("zb", "zc")
FAR = ("za", "zb")

VMEM = pl.BlockSpec(memory_space=pltpu.VMEM)
PLAIN = pl.BlockSpec(memory_space=pltpu.VMEM)
SMEM = pl.BlockSpec(memory_space=pltpu.SMEM)
ANY = pl.BlockSpec(memory_space=pl.ANY)


def call(kernel, outs, name, specs=None, scratch=(), flops=0, limit=16):
    def run(*args):
        in_specs = specs if specs is not None else [VMEM] * len(args)
        placed = [placed_for(arg, spec) for arg, spec in zip(args, in_specs)]
        return pl.pallas_call(
            kernel,
            out_shape=[o[0] for o in outs],
            in_specs=in_specs,
            out_specs=[o[1] for o in outs],
            scratch_shapes=list(scratch),
            interpret=INTERPRET,
            name=name,
            compiler_params=pltpu.CompilerParams(vmem_limit_bytes=limit << 20 if limit else None),
            cost_estimate=pl.CostEstimate(flops=flops, bytes_accessed=0, transcendentals=0),
        )(*placed)

    return run


def placed_for(arg, spec):
    if INTERPRET or all(spec is not kind for kind in (VMEM, ANY)):
        return arg
    return pltpu.with_memory_space_constraint(arg, pltpu.VMEM if spec is VMEM else pltpu.HBM)


def fast(dims, kind):
    return (jax.ShapeDtypeStruct(dims, kind) if INTERPRET else pltpu.VMEM(dims, kind), VMEM)


def slow(dims, kind):
    return (jax.ShapeDtypeStruct(dims, kind), VMEM)


def dot(a, b, dims):
    return lax.dot_general(a, b, (dims, ((), ())), preferred_element_type=F32)


def pack_kernel(key, value, *refs):
    *inputs, logs, rest, message = refs
    for at, ref in enumerate(inputs):
        for core in range(2):
            to = core * COLUMNS + at * HEAD
            rest[:, to : to + HEAD] = ref[:, core * HEAD : (core + 1) * HEAD]
    shard = key.shape[0]
    for core in range(2):
        message[core, :shard, :HEAD] = key[:, core * HEAD : (core + 1) * HEAD]
        message[core, :shard, HEAD:] = value[:, core * HEAD : (core + 1) * HEAD]
        lines = [logs[core : core + 1, at : at + 2 * HEAD] for at in range(0, logs.shape[1], 2 * HEAD)]
        line = jnp.concatenate(lines, axis=0)
        high = line.astype(BF16).astype(F32)
        middle = (line - high).astype(BF16).astype(F32)
        low = line - high - middle
        filler = jnp.zeros((EXTRA - 3 * len(lines), 2 * HEAD), F32)
        message[core, shard:, :] = jnp.concatenate([high, middle, low, filler], axis=0).astype(BF16)


def logs_of(rows, lines):
    rows = rows.astype(F32)
    return rows[:lines] + rows[lines : 2 * lines] + rows[2 * lines : 3 * lines]


def norm_kernel(tokens, gain, out):
    values = tokens[...].astype(F32)
    scale = lax.rsqrt(jnp.mean(values * values, axis=-1, keepdims=True) + EPSILON)
    normed = (values * scale * gain[...].astype(F32)[None, :]).astype(BF16)
    for copy in range(out.shape[0]):
        out[copy] = normed


def rotated(head, cosine, sine):
    return head * cosine + pltpu.roll(head, HALF, 1) * sine


def kv_kernel(
    pair, x, same, low, high, own, cos_far, sin_far, cos_near, sin_near, k_out, v_out, cosine, sine, decay, column, totals, message, weight
):
    rows, width = x.shape[0] * x.shape[1], x.shape[2]
    half = low.shape[0]
    shard = own.shape[1] - EXTRA
    lines = rows // 2 // (2 * HEAD)

    pieces = []
    for core in range(2):
        logs = logs_of(own[core, shard:, :], lines)
        for line in range(lines):
            pieces += [logs[line : line + 1, :HEAD], logs[line : line + 1, HEAD:]]
    logs = jnp.concatenate(pieces, axis=0)
    upper = lax.broadcasted_iota(jnp.int32, (HEAD, HEAD), 0) <= lax.broadcasted_iota(jnp.int32, (HEAD, HEAD), 1)
    inner = lax.dot_general(
        logs,
        upper.astype(F32),
        (((1,), (0,)), ((), ())),
        precision=lax.Precision.HIGHEST,
        preferred_element_type=F32,
    )
    before = jnp.zeros((1, 1), F32)
    added = []
    for at in range(len(pieces)):
        added.append(inner[at : at + 1] + before)
        before = before + inner[at : at + 1, HEAD - 1 :]
    cumulative = jnp.concatenate(added, axis=0)
    decay[...] = cumulative
    filler = jnp.zeros((HEAD - len(pieces), HEAD), F32)
    column[...] = jnp.concatenate([cumulative, filler], axis=0).T
    total = before

    mine, others = pair[0], 1 - pair[0]
    for source, first, place in ((same, 0, mine), (low, 0, others), (high, half, others)):
        for at_far in range(source.shape[0]):
            chip = 2 * (first + at_far) + place
            log_total = jnp.zeros((1, 1), F32)
            for core in range(2):
                at = core * (shard + EXTRA)
                to = pl.multiple_of((2 * chip + core) * shard, shard)
                weight[pl.ds(to, shard), :] = source[at_far, at : at + shard, :]
                logs = logs_of(source[at_far, at + shard : at + shard + EXTRA, :], lines)
                log_total = log_total + jnp.sum(logs, axis=(0, 1), keepdims=True)
            totals[pl.ds(chip, 1), :] = jnp.broadcast_to(log_total, (1, HEAD))

    state = jnp.zeros((HEAD, HEAD), F32)
    for i in range(rows // BLOCK):
        at = pl.ds(i * BLOCK, BLOCK)
        cos_at = cos_far[i : i + 1, :] * cos_near[...] - sin_far[i : i + 1, :] * sin_near[...]
        sin_at = sin_far[i : i + 1, :] * cos_near[...] + cos_far[i : i + 1, :] * sin_near[...]
        first = lax.broadcasted_iota(jnp.int32, sin_at.shape, 1) < HALF
        sin_at = jnp.where(first, -sin_at, sin_at)
        cosine[at, :] = cos_at
        sine[at, :] = sin_at
        both = dot(block_rows(x, i), weight[...], ((1,), (0,))).astype(BF16)
        key = rotated(both[:, :HEAD].astype(F32), cos_at, sin_at) * HEAD ** (-0.5)
        k_out[at, :] = key.astype(BF16)
        value = both[:, HEAD:]
        v_out[at, :] = value
        here = block_column(column, i)
        faded = (key * jnp.exp(total - here)).astype(BF16)
        state = state + dot(faded, value, ((0,), (0,)))
    for copy in range(message.shape[0]):
        message[copy] = state.astype(BF16)


def block_rows(x, i):
    per = BLOCK // x.shape[1]
    return x[i * per : (i + 1) * per].reshape(BLOCK, x.shape[2])


def block_column(column, i):
    per = BLOCK // HEAD
    return jnp.concatenate([column[:, per * i + j : per * i + j + 1] for j in range(per)], axis=0)


def near_kernel(place, block, totals, gathered, message, before, fade, scratch):
    own = place[0]
    near = gathered.shape[0]
    run = jnp.zeros((HEAD, HEAD), F32)
    passed = jnp.zeros((1, HEAD), F32)
    kept, kept_passed = run, passed
    for at in range(near):
        kept = jnp.where(own == at, run, kept)
        kept_passed = jnp.where(own == at, passed, kept_passed)
        log_total = totals[pl.ds(block[0] * near + at, 1), :]
        run = jnp.exp(log_total) * run + gathered[at].astype(F32)
        passed = passed + log_total
    before[...] = kept
    fade[...] = jnp.broadcast_to(jnp.exp(kept_passed), fade.shape)
    scratch[...] = run
    share = HEAD // near
    part = scratch[pl.ds(pl.multiple_of(own * share, share), share), :].astype(BF16)
    for copy in range(message.shape[0]):
        message[copy] = part


def far_kernel(place, totals, gathered, message):
    own = place[0]
    near, share = message.shape[:2]
    run = jnp.zeros((share, HEAD), F32)
    kept = run
    for at in range(gathered.shape[0]):
        kept = jnp.where(own == at, run, kept)
        log_total = jnp.sum(totals[at * near : (at + 1) * near, :], axis=0, keepdims=True)
        run = jnp.exp(log_total) * run + gathered[at].astype(F32)
    for copy in range(near):
        message[copy] = kept.astype(BF16)


def branch_kernel(
    core,
    weights,
    x,
    halo,
    cosine,
    sine,
    decay,
    column,
    keys,
    values,
    base,
    before,
    fade,
    taps,
    branches,
    out_weight,
    weight,
    semaphores,
):
    rows = x.shape[0] * x.shape[1]
    own = core[0]
    start_at = pl.multiple_of(own * COLUMNS, HEAD)
    other_at = pl.multiple_of((1 - own) * COLUMNS, HEAD)
    piece = weight.shape[0] // PIECES
    copies = [
        *(
            pltpu.make_async_copy(
                weights.at[pl.ds(at, piece), pl.ds(start_at, PROJECTED)],
                weight.at[pl.ds(at, piece), :],
                semaphores.at[2 + at // piece],
            )
            for at in range(0, weight.shape[0], piece)
        ),
        pltpu.make_async_copy(
            weights.at[:, pl.ds(start_at + PROJECTED, 2 * HEAD)], out_weight.at[0], semaphores.at[0]
        ),
        pltpu.make_async_copy(
            weights.at[:, pl.ds(other_at + PROJECTED, 2 * HEAD)], out_weight.at[1], semaphores.at[1]
        ),
    ]
    for copy in copies:
        copy.start()
    incoming = jnp.concatenate([base[at].astype(F32) for at in range(base.shape[0])], axis=0)
    state = fade[0:1, :] * incoming + before[...]
    row = lax.broadcasted_iota(jnp.int32, (BLOCK, HEAD), 0)
    causal = lax.broadcasted_iota(jnp.int32, (BLOCK, BLOCK), 0) >= lax.broadcasted_iota(
        jnp.int32, (BLOCK, BLOCK), 1
    )
    tap = jnp.where(own == 0, taps[:, :HEAD].astype(F32), taps[:, HEAD:].astype(F32))
    start = jnp.zeros((1, 1), F32)
    per = BLOCK // HEAD
    first = jnp.zeros((BLOCK, PROJECTED), F32)
    for at in range(PIECES):
        copies[at].wait()
        cut = slice(at * piece, (at + 1) * piece)
        first = first + dot(block_rows(x, 0)[:, cut], weight[cut, :], ((1,), (0,)))
    rim = dot(halo[...], weight[:, HEAD : 3 * HEAD], ((1,), (0,))).astype(BF16).astype(F32)
    tail = (rim[:, :HEAD] * rim[:, HEAD:])[RIM - 8 :]
    for i in range(rows // BLOCK):
        at = pl.ds(i * BLOCK, BLOCK)
        half = (i * BLOCK) // (rows // 2)
        place = slice(i * BLOCK - half * (rows // 2), (i + 1) * BLOCK - half * (rows // 2))
        slot = jnp.where(own == half, 0, 1)
        projected = (dot(block_rows(x, i), weight[...], ((1,), (0,))) if i else first).astype(BF16)
        outer = projected[:, :HEAD].astype(F32)
        mixed = projected[:, HEAD : 2 * HEAD].astype(F32) * projected[:, 2 * HEAD : 3 * HEAD].astype(F32)
        one = jnp.where(row == 0, tail[7:8], pltpu.roll(mixed, 1, 0))
        two = jnp.where(row == 0, tail[6:7], jnp.where(row == 1, tail[7:8], pltpu.roll(mixed, 2, 0)))
        conv = tap[0:1] * two + tap[1:2] * one + tap[2:3] * mixed
        tail = mixed[BLOCK - 8 :]
        branches[slot, place, :HEAD] = (outer * conv).astype(BF16)

        query = rotated(projected[:, 3 * HEAD : 4 * HEAD].astype(F32), cosine[at, :], sine[at, :])
        query = query.astype(BF16)
        key, value = keys[at, :], values[at, :]
        here = block_column(column, i)
        line = jnp.concatenate([decay[per * i + j : per * i + j + 1, :] for j in range(per)], axis=1)
        spread = jnp.where(causal, here - line, 0.0)
        scores = jnp.where(causal, dot(query, key, ((1,), (1,))) * jnp.exp(spread), 0.0)
        within = dot(scores.astype(BF16), value, ((1,), (0,)))
        across = dot(query, state.astype(BF16), ((1,), (0,))) * jnp.exp(here - start)
        retained = within + across
        end = line[:, BLOCK - 1 :]
        faded = (key.astype(F32) * jnp.exp(end - here)).astype(BF16)
        state = jnp.exp(end - start) * state + dot(faded, value, ((0,), (0,)))
        start = end
        normed = retained * lax.rsqrt(jnp.mean(retained * retained, axis=-1, keepdims=True) + EPSILON)
        gate = projected[:, 4 * HEAD :].astype(F32)
        ret_branch = (normed * (gate / (1.0 + jnp.exp(-gate)))).astype(BF16)

        branches[slot, place, HEAD:] = ret_branch

    copies[PIECES].wait()
    copies[PIECES + 1].wait()


def out_kernel(mine, theirs, weight, out):
    parts, rows = out.shape[0], out.shape[1]
    step = 512
    for column in range(0, out.shape[2], step):
        at = pl.ds(column, step)
        total = dot(mine[0], weight[0, at, :], ((1,), (1,))) + dot(theirs[1], weight[1, at, :], ((1,), (1,)))
        total = total.astype(BF16)
        for part in range(parts):
            out[part, :, column : column + step] = total[part * rows : (part + 1) * rows]


def exchanged(x, axes):
    return lax.all_to_all(x, axes, 0, 0, tiled=True)


def body(
    tokens,
    norm_gain,
    conv_outer_weight,
    conv_inner_weight,
    conv_input_weight,
    query_matrix,
    key_weight,
    value_weight,
    gate_weight,
    conv_taps,
    conv_out_weight,
    ret_out_weight,
    log_decay,
):
    own_rows, width = tokens.shape
    tp = lax.axis_size("tp")
    chip = lax.axis_index(CHIPS)
    core = lax.axis_index("core")
    chips = lax.axis_size(CHIPS)
    near, far = lax.axis_size(NEAR), lax.axis_size("za")
    rows = 2 * tp * own_rows
    shard = key_weight.shape[0]

    rest, message = call(
        pack_kernel,
        [slow((shard, 2 * COLUMNS), BF16), fast((2, shard + EXTRA, 2 * HEAD), BF16)],
        "pack",
        specs=[PLAIN] * 10,
        limit=None,
    )(
        key_weight,
        value_weight,
        conv_outer_weight,
        conv_inner_weight,
        conv_input_weight,
        query_matrix,
        gate_weight,
        conv_out_weight.T,
        ret_out_weight.T,
        log_decay.T,
    )
    weights = lax.all_gather(rest, STRETCHES, axis=0, tiled=True)

    own = exchanged(message, "core")
    same = lax.all_gather(own.reshape(2 * (shard + EXTRA), 2 * HEAD), FAR)
    half = same.shape[0] // 2
    low = lax.ppermute(same[:half], CHIPS, [(i, (i - 1) % chips) for i in range(chips)])
    high = lax.ppermute(same[half:], CHIPS, [(i, (i + 1) % chips) for i in range(chips)])

    (normed,) = call(norm_kernel, [slow((2 * tp, own_rows, width), BF16)], "norm", specs=[PLAIN] * 2, limit=None)(
        tokens, norm_gain
    )
    x = exchanged(normed, ("core", "tp"))
    halo = lax.ppermute(x[-1, own_rows - RIM :], CHIPS, [(i, i + 1) for i in range(chips - 1)])

    inv_freq = ROTARY_BASE ** (-jnp.arange(HALF, dtype=F32) / HALF)
    inv_freq = jnp.concatenate([inv_freq, inv_freq])[None, :]
    far_angle = ((chip * rows).astype(F32) + BLOCK * jnp.arange(8, dtype=F32))[:, None] * inv_freq
    near_angle = jnp.arange(BLOCK, dtype=F32)[:, None] * inv_freq

    keys, values, cosine, sine, decay, column, totals, message = call(
        kv_kernel,
        [
            fast((rows, HEAD), BF16),
            fast((rows, HEAD), BF16),
            fast((rows, HEAD), F32),
            fast((rows, HEAD), F32),
            fast((rows // HEAD, HEAD), F32),
            fast((HEAD, HEAD), F32),
            fast((chips, HEAD), F32),
            fast((near, HEAD, HEAD), BF16),
        ],
        "kv",
        specs=[SMEM] + [VMEM] * 9,
        scratch=[pltpu.VMEM((width, 2 * HEAD), BF16)],
        flops=4 * rows * width * HEAD,
    )(lax.axis_index("zc").reshape(1), x, same, low, high, own, jnp.cos(far_angle), jnp.sin(far_angle), jnp.cos(near_angle), jnp.sin(near_angle))

    share = HEAD // near
    block = lax.axis_index("za").reshape(1)
    message, before, fade = call(
        near_kernel,
        [fast((far, share, HEAD), BF16), fast((HEAD, HEAD), F32), fast((8, HEAD), F32)],
        "near",
        specs=[SMEM, SMEM, VMEM, VMEM],
        scratch=[pltpu.VMEM((HEAD, HEAD), F32)],
    )(lax.axis_index(NEAR).reshape(1), block, totals, exchanged(message, NEAR))
    (message,) = call(far_kernel, [fast((near, share, HEAD), BF16)], "far", specs=[SMEM, VMEM, VMEM])(
        block, totals, exchanged(message, "za")
    )
    base = exchanged(message, NEAR)

    branches, out_weight = call(
        branch_kernel,
        [fast((2, rows // 2, 2 * HEAD), BF16), fast((2, width, 2 * HEAD), BF16)],
        "branch",
        specs=[SMEM, ANY] + [VMEM] * 12,
        scratch=[pltpu.VMEM((width, PROJECTED), BF16), pltpu.SemaphoreType.DMA((PIECES + 2,))],
        flops=10 * rows * width * HEAD,
    )(
        core.reshape(1),
        weights,
        x,
        halo,
        cosine,
        sine,
        decay,
        column,
        keys,
        values,
        base,
        before,
        fade,
        conv_taps,
    )
    theirs = lax.ppermute(branches, "core", [(0, 1), (1, 0)])
    (partial,) = call(out_kernel, [slow((tp, own_rows, width), BF16)], "out", flops=rows * width * 4 * HEAD)(
        branches, theirs, out_weight
    )
    return lax.psum_scatter(partial.reshape(tp * own_rows, width), "tp", scatter_dimension=0, tiled=True)


def solution(mesh):
    groups, stretches, tp = mesh.devices.shape
    chips = stretches // 2
    fine = Mesh(
        mesh.devices.reshape(groups, chips // 4, 2, 2, 2, tp), ("grp", "za", "zb", "zc", "core", "tp")
    )
    columns = P(STRETCHES, "tp")
    placed = (
        P(("grp", *STRETCHES, "tp"), None),
        P(),
        *([columns] * 7),
        P(None, "tp"),
        P("tp", STRETCHES),
        P("tp", STRETCHES),
        P(("grp", *STRETCHES), "tp"),
    )
    return jax.shard_map(
        body, mesh=fine, in_specs=placed, out_specs=P(("grp", *STRETCHES, "tp"), None), check_vma=False
    )
```

```python
import jax
import jax.numpy as jnp
from jax import lax
from jax.experimental import pallas as pl
from jax.experimental.pallas import tpu as pltpu
from jax.sharding import Mesh, PartitionSpec as P

HEAD = 128
HALF = HEAD // 2
CONV_K = 3
EPSILON = 1e-06
ROTARY_BASE = 10000.0
BLOCK = 256
EXTRA = 8
RIM = 16
PROJECTED = 5 * HEAD
PIECES = 4
COLUMNS = 7 * HEAD
INTERPRET = False

BF16 = jnp.bfloat16
F32 = jnp.float32
CHIPS = ("za", "zb", "zc")
STRETCHES = ("za", "zb", "zc", "core")
NEAR = ("zb", "zc")
FAR = ("za", "zb")

VMEM = pl.BlockSpec(memory_space=pltpu.VMEM)
PLAIN = pl.BlockSpec(memory_space=pltpu.VMEM)
SMEM = pl.BlockSpec(memory_space=pltpu.SMEM)
ANY = pl.BlockSpec(memory_space=pl.ANY)


def call(kernel, outs, name, specs=None, scratch=(), flops=0, limit=16):
    def run(*args):
        in_specs = specs if specs is not None else [VMEM] * len(args)
        placed = [placed_for(arg, spec) for arg, spec in zip(args, in_specs)]
        return pl.pallas_call(
            kernel,
            out_shape=[o[0] for o in outs],
            in_specs=in_specs,
            out_specs=[o[1] for o in outs],
            scratch_shapes=list(scratch),
            interpret=INTERPRET,
            name=name,
            compiler_params=pltpu.CompilerParams(vmem_limit_bytes=limit << 20 if limit else None),
            cost_estimate=pl.CostEstimate(flops=flops, bytes_accessed=0, transcendentals=0),
        )(*placed)

    return run


def placed_for(arg, spec):
    if INTERPRET or all(spec is not kind for kind in (VMEM, ANY)):
        return arg
    return pltpu.with_memory_space_constraint(arg, pltpu.VMEM if spec is VMEM else pltpu.HBM)


def fast(dims, kind):
    return (jax.ShapeDtypeStruct(dims, kind) if INTERPRET else pltpu.VMEM(dims, kind), VMEM)


def slow(dims, kind):
    return (jax.ShapeDtypeStruct(dims, kind), VMEM)


def dot(a, b, dims):
    return lax.dot_general(a, b, (dims, ((), ())), preferred_element_type=F32)


def pack_kernel(key, value, *refs):
    *inputs, logs, rest, message = refs
    for at, ref in enumerate(inputs):
        for core in range(2):
            to = core * COLUMNS + at * HEAD
            rest[:, to : to + HEAD] = ref[:, core * HEAD : (core + 1) * HEAD]
    shard = key.shape[0]
    for core in range(2):
        message[core, :shard, :HEAD] = key[:, core * HEAD : (core + 1) * HEAD]
        message[core, :shard, HEAD:] = value[:, core * HEAD : (core + 1) * HEAD]
        lines = [logs[core : core + 1, at : at + 2 * HEAD] for at in range(0, logs.shape[1], 2 * HEAD)]
        line = jnp.concatenate(lines, axis=0)
        high = line.astype(BF16).astype(F32)
        middle = (line - high).astype(BF16).astype(F32)
        low = line - high - middle
        filler = jnp.zeros((EXTRA - 3 * len(lines), 2 * HEAD), F32)
        message[core, shard:, :] = jnp.concatenate([high, middle, low, filler], axis=0).astype(BF16)


def logs_of(rows, lines):
    rows = rows.astype(F32)
    return rows[:lines] + rows[lines : 2 * lines] + rows[2 * lines : 3 * lines]


def norm_kernel(tokens, gain, out):
    values = tokens[...].astype(F32)
    scale = lax.rsqrt(jnp.mean(values * values, axis=-1, keepdims=True) + EPSILON)
    normed = (values * scale * gain[...].astype(F32)[None, :]).astype(BF16)
    for copy in range(out.shape[0]):
        out[copy] = normed


def rotated(head, cosine, sine):
    return head * cosine + pltpu.roll(head, HALF, 1) * sine


def kv_kernel(
    pair, x, same, low, high, own, cos_far, sin_far, cos_near, sin_near, k_out, v_out, cosine, sine, decay, column, totals, message, last, x_kept, weight, semaphores
):
    per = BLOCK // x.shape[1]
    copies = [
        pltpu.make_async_copy(x.at[pl.ds(i * per, per)], x_kept.at[pl.ds(i * per, per)], semaphores.at[i])
        for i in range(x.shape[0] // per)
    ]
    for copy in copies:
        copy.start()
    rows, width = x.shape[0] * x.shape[1], x.shape[2]
    half = low.shape[0]
    shard = own.shape[1] - EXTRA
    lines = rows // 2 // (2 * HEAD)

    pieces = []
    for core in range(2):
        logs = logs_of(own[core, shard:, :], lines)
        for line in range(lines):
            pieces += [logs[line : line + 1, :HEAD], logs[line : line + 1, HEAD:]]
    logs = jnp.concatenate(pieces, axis=0)
    upper = lax.broadcasted_iota(jnp.int32, (HEAD, HEAD), 0) <= lax.broadcasted_iota(jnp.int32, (HEAD, HEAD), 1)
    inner = lax.dot_general(
        logs,
        upper.astype(F32),
        (((1,), (0,)), ((), ())),
        precision=lax.Precision.HIGHEST,
        preferred_element_type=F32,
    )
    before = jnp.zeros((1, 1), F32)
    added = []
    for at in range(len(pieces)):
        added.append(inner[at : at + 1] + before)
        before = before + inner[at : at + 1, HEAD - 1 :]
    cumulative = jnp.concatenate(added, axis=0)
    decay[...] = cumulative
    filler = jnp.zeros((HEAD - len(pieces), HEAD), F32)
    column[...] = jnp.concatenate([cumulative, filler], axis=0).T
    total = before

    mine, others = pair[0], 1 - pair[0]
    for source, first, place in ((same, 0, mine), (low, 0, others), (high, half, others)):
        for at_far in range(source.shape[0]):
            chip = 2 * (first + at_far) + place
            log_total = jnp.zeros((1, 1), F32)
            for core in range(2):
                at = core * (shard + EXTRA)
                to = pl.multiple_of((2 * chip + core) * shard, shard)
                weight[pl.ds(to, shard), :] = source[at_far, at : at + shard, :]
                logs = logs_of(source[at_far, at + shard : at + shard + EXTRA, :], lines)
                log_total = log_total + jnp.sum(logs, axis=(0, 1), keepdims=True)
            totals[pl.ds(chip, 1), :] = jnp.broadcast_to(log_total, (1, HEAD))

    state = jnp.zeros((HEAD, HEAD), F32)
    for i in range(rows // BLOCK):
        at = pl.ds(i * BLOCK, BLOCK)
        cos_at = cos_far[i : i + 1, :] * cos_near[...] - sin_far[i : i + 1, :] * sin_near[...]
        sin_at = sin_far[i : i + 1, :] * cos_near[...] + cos_far[i : i + 1, :] * sin_near[...]
        first = lax.broadcasted_iota(jnp.int32, sin_at.shape, 1) < HALF
        sin_at = jnp.where(first, -sin_at, sin_at)
        cosine[at, :] = cos_at
        sine[at, :] = sin_at
        copies[i].wait()
        both = dot(block_rows(x_kept, i), weight[...], ((1,), (0,))).astype(BF16)
        key = rotated(both[:, :HEAD].astype(F32), cos_at, sin_at) * HEAD ** (-0.5)
        k_out[at, :] = key.astype(BF16)
        value = both[:, HEAD:]
        v_out[at, :] = value
        here = block_column(column, i)
        faded = (key * jnp.exp(total - here)).astype(BF16)
        state = state + dot(faded, value, ((0,), (0,)))
    for copy in range(message.shape[0]):
        message[copy] = state.astype(BF16)
    last[...] = x_kept[x.shape[0] - 1, x.shape[1] - RIM :, :]


def block_rows(x, i):
    per = BLOCK // x.shape[1]
    return x[i * per : (i + 1) * per].reshape(BLOCK, x.shape[2])


def block_column(column, i):
    per = BLOCK // HEAD
    return jnp.concatenate([column[:, per * i + j : per * i + j + 1] for j in range(per)], axis=0)


def near_kernel(place, block, totals, gathered, message, before, fade, scratch):
    own = place[0]
    near = gathered.shape[0]
    run = jnp.zeros((HEAD, HEAD), F32)
    passed = jnp.zeros((1, HEAD), F32)
    kept, kept_passed = run, passed
    for at in range(near):
        kept = jnp.where(own == at, run, kept)
        kept_passed = jnp.where(own == at, passed, kept_passed)
        log_total = totals[pl.ds(block[0] * near + at, 1), :]
        run = jnp.exp(log_total) * run + gathered[at].astype(F32)
        passed = passed + log_total
    before[...] = kept
    fade[...] = jnp.broadcast_to(jnp.exp(kept_passed), fade.shape)
    scratch[...] = run
    share = HEAD // near
    part = scratch[pl.ds(pl.multiple_of(own * share, share), share), :].astype(BF16)
    for copy in range(message.shape[0]):
        message[copy] = part


def far_kernel(place, totals, gathered, message):
    own = place[0]
    near, share = message.shape[:2]
    run = jnp.zeros((share, HEAD), F32)
    kept = run
    for at in range(gathered.shape[0]):
        kept = jnp.where(own == at, run, kept)
        log_total = jnp.sum(totals[at * near : (at + 1) * near, :], axis=0, keepdims=True)
        run = jnp.exp(log_total) * run + gathered[at].astype(F32)
    for copy in range(near):
        message[copy] = kept.astype(BF16)


def branch_kernel(
    core,
    weights,
    x_far,
    halo,
    cosine,
    sine,
    decay,
    column,
    keys,
    values,
    base,
    before,
    fade,
    taps,
    branches,
    out_weight,
    x,
    weight,
    semaphores,
):
    rows = x.shape[0] * x.shape[1]
    blocks = rows // BLOCK
    own = core[0]
    start_at = pl.multiple_of(own * COLUMNS, HEAD)
    other_at = pl.multiple_of((1 - own) * COLUMNS, HEAD)
    piece = weight.shape[0] // PIECES
    copies = [
        *(
            pltpu.make_async_copy(
                weights.at[pl.ds(at, piece), pl.ds(start_at, PROJECTED)],
                weight.at[pl.ds(at, piece), :],
                semaphores.at[2 + at // piece],
            )
            for at in range(0, weight.shape[0], piece)
        ),
        pltpu.make_async_copy(
            weights.at[:, pl.ds(start_at + PROJECTED, 2 * HEAD)], out_weight.at[0], semaphores.at[0]
        ),
        pltpu.make_async_copy(
            weights.at[:, pl.ds(other_at + PROJECTED, 2 * HEAD)], out_weight.at[1], semaphores.at[1]
        ),
    ]
    per_block = x.shape[0] // blocks
    x_copies = [
        pltpu.make_async_copy(
            x_far.at[pl.ds(i * per_block, per_block)],
            x.at[pl.ds(i * per_block, per_block)],
            semaphores.at[PIECES + 2 + i],
        )
        for i in range(blocks)
    ]
    x_copies[0].start()
    for copy in copies[:PIECES]:
        copy.start()
    for copy in x_copies[1:]:
        copy.start()
    incoming = jnp.concatenate([base[at].astype(F32) for at in range(base.shape[0])], axis=0)
    state = fade[0:1, :] * incoming + before[...]
    row = lax.broadcasted_iota(jnp.int32, (BLOCK, HEAD), 0)
    causal = lax.broadcasted_iota(jnp.int32, (BLOCK, BLOCK), 0) >= lax.broadcasted_iota(
        jnp.int32, (BLOCK, BLOCK), 1
    )
    tap = jnp.where(own == 0, taps[:, :HEAD].astype(F32), taps[:, HEAD:].astype(F32))
    start = jnp.zeros((1, 1), F32)
    per = BLOCK // HEAD
    first = jnp.zeros((BLOCK, PROJECTED), F32)
    x_copies[0].wait()
    for at in range(PIECES):
        copies[at].wait()
        cut = slice(at * piece, (at + 1) * piece)
        first = first + dot(block_rows(x, 0)[:, cut], weight[cut, :], ((1,), (0,)))
    for copy in copies[PIECES:]:
        copy.start()
    rim = dot(halo[...], weight[:, HEAD : 3 * HEAD], ((1,), (0,))).astype(BF16).astype(F32)
    tail = (rim[:, :HEAD] * rim[:, HEAD:])[RIM - 8 :]
    for i in range(rows // BLOCK):
        at = pl.ds(i * BLOCK, BLOCK)
        half = (i * BLOCK) // (rows // 2)
        place = slice(i * BLOCK - half * (rows // 2), (i + 1) * BLOCK - half * (rows // 2))
        slot = jnp.where(own == half, 0, 1)
        if i:
            x_copies[i].wait()
        projected = (dot(block_rows(x, i), weight[...], ((1,), (0,))) if i else first).astype(BF16)
        outer = projected[:, :HEAD].astype(F32)
        mixed = projected[:, HEAD : 2 * HEAD].astype(F32) * projected[:, 2 * HEAD : 3 * HEAD].astype(F32)
        one = jnp.where(row == 0, tail[7:8], pltpu.roll(mixed, 1, 0))
        two = jnp.where(row == 0, tail[6:7], jnp.where(row == 1, tail[7:8], pltpu.roll(mixed, 2, 0)))
        conv = tap[0:1] * two + tap[1:2] * one + tap[2:3] * mixed
        tail = mixed[BLOCK - 8 :]
        branches[slot, place, :HEAD] = (outer * conv).astype(BF16)

        query = rotated(projected[:, 3 * HEAD : 4 * HEAD].astype(F32), cosine[at, :], sine[at, :])
        query = query.astype(BF16)
        key, value = keys[at, :], values[at, :]
        here = block_column(column, i)
        line = jnp.concatenate([decay[per * i + j : per * i + j + 1, :] for j in range(per)], axis=1)
        spread = jnp.where(causal, here - line, 0.0)
        scores = jnp.where(causal, dot(query, key, ((1,), (1,))) * jnp.exp(spread), 0.0)
        within = dot(scores.astype(BF16), value, ((1,), (0,)))
        across = dot(query, state.astype(BF16), ((1,), (0,))) * jnp.exp(here - start)
        retained = within + across
        end = line[:, BLOCK - 1 :]
        faded = (key.astype(F32) * jnp.exp(end - here)).astype(BF16)
        state = jnp.exp(end - start) * state + dot(faded, value, ((0,), (0,)))
        start = end
        normed = retained * lax.rsqrt(jnp.mean(retained * retained, axis=-1, keepdims=True) + EPSILON)
        gate = projected[:, 4 * HEAD :].astype(F32)
        ret_branch = (normed * (gate / (1.0 + jnp.exp(-gate)))).astype(BF16)

        branches[slot, place, HEAD:] = ret_branch

    copies[PIECES].wait()
    copies[PIECES + 1].wait()


def out_kernel(mine, theirs, weight, out):
    parts, rows = out.shape[0], out.shape[1]
    step = 512
    for column in range(0, out.shape[2], step):
        at = pl.ds(column, step)
        total = dot(mine[0], weight[0, at, :], ((1,), (1,))) + dot(theirs[1], weight[1, at, :], ((1,), (1,)))
        total = total.astype(BF16)
        for part in range(parts):
            out[part, :, column : column + step] = total[part * rows : (part + 1) * rows]


def sum_kernel(parts, out):
    total = parts[0].astype(F32)
    for at in range(1, parts.shape[0]):
        total = total + parts[at].astype(F32)
    out[...] = total.astype(BF16)


def exchanged(x, axes):
    return lax.all_to_all(x, axes, 0, 0, tiled=True)


def body(
    tokens,
    norm_gain,
    conv_outer_weight,
    conv_inner_weight,
    conv_input_weight,
    query_matrix,
    key_weight,
    value_weight,
    gate_weight,
    conv_taps,
    conv_out_weight,
    ret_out_weight,
    log_decay,
):
    own_rows, width = tokens.shape
    tp = lax.axis_size("tp")
    chip = lax.axis_index(CHIPS)
    core = lax.axis_index("core")
    chips = lax.axis_size(CHIPS)
    near, far = lax.axis_size(NEAR), lax.axis_size("za")
    rows = 2 * tp * own_rows
    shard = key_weight.shape[0]

    rest, message = call(
        pack_kernel,
        [slow((shard, 2 * COLUMNS), BF16), fast((2, shard + EXTRA, 2 * HEAD), BF16)],
        "pack",
        specs=[PLAIN] * 10,
        limit=None,
    )(
        key_weight,
        value_weight,
        conv_outer_weight,
        conv_inner_weight,
        conv_input_weight,
        query_matrix,
        gate_weight,
        conv_out_weight.T,
        ret_out_weight.T,
        log_decay.T,
    )
    weights = lax.all_gather(rest, STRETCHES, axis=0, tiled=True)

    own = exchanged(message, "core")
    same = lax.all_gather(own.reshape(2 * (shard + EXTRA), 2 * HEAD), FAR)
    half = same.shape[0] // 2
    low = lax.ppermute(same[:half], CHIPS, [(i, (i - 1) % chips) for i in range(chips)])
    high = lax.ppermute(same[half:], CHIPS, [(i, (i + 1) % chips) for i in range(chips)])

    (normed,) = call(norm_kernel, [slow((2 * tp, own_rows, width), BF16)], "norm", specs=[PLAIN] * 2, limit=None)(
        tokens, norm_gain
    )
    x = exchanged(normed, ("core", "tp"))

    inv_freq = ROTARY_BASE ** (-jnp.arange(HALF, dtype=F32) / HALF)
    inv_freq = jnp.concatenate([inv_freq, inv_freq])[None, :]
    far_angle = ((chip * rows).astype(F32) + BLOCK * jnp.arange(8, dtype=F32))[:, None] * inv_freq
    near_angle = jnp.arange(BLOCK, dtype=F32)[:, None] * inv_freq

    keys, values, cosine, sine, decay, column, totals, message, last = call(
        kv_kernel,
        [
            fast((rows, HEAD), BF16),
            fast((rows, HEAD), BF16),
            fast((rows, HEAD), F32),
            fast((rows, HEAD), F32),
            fast((rows // HEAD, HEAD), F32),
            fast((HEAD, HEAD), F32),
            fast((chips, HEAD), F32),
            fast((near, HEAD, HEAD), BF16),
            fast((RIM, width), BF16),
        ],
        "kv",
        specs=[SMEM, ANY] + [VMEM] * 8,
        scratch=[
            pltpu.VMEM(x.shape, BF16),
            pltpu.VMEM((width, 2 * HEAD), BF16),
            pltpu.SemaphoreType.DMA((rows // BLOCK,)),
        ],
        flops=4 * rows * width * HEAD,
    )(lax.axis_index("zc").reshape(1), x, same, low, high, own, jnp.cos(far_angle), jnp.sin(far_angle), jnp.cos(near_angle), jnp.sin(near_angle))

    halo = lax.ppermute(last, CHIPS, [(i, i + 1) for i in range(chips - 1)])

    share = HEAD // near
    block = lax.axis_index("za").reshape(1)
    message, before, fade = call(
        near_kernel,
        [fast((far, share, HEAD), BF16), fast((HEAD, HEAD), F32), fast((8, HEAD), F32)],
        "near",
        specs=[SMEM, SMEM, VMEM, VMEM],
        scratch=[pltpu.VMEM((HEAD, HEAD), F32)],
    )(lax.axis_index(NEAR).reshape(1), block, totals, exchanged(message, NEAR))
    (message,) = call(far_kernel, [fast((near, share, HEAD), BF16)], "far", specs=[SMEM, VMEM, VMEM])(
        block, totals, exchanged(message, "za")
    )
    base = exchanged(message, NEAR)

    branches, out_weight = call(
        branch_kernel,
        [fast((2, rows // 2, 2 * HEAD), BF16), fast((2, width, 2 * HEAD), BF16)],
        "branch",
        specs=[SMEM, ANY, ANY] + [VMEM] * 11,
        scratch=[
            pltpu.VMEM(x.shape, BF16),
            pltpu.VMEM((width, PROJECTED), BF16),
            pltpu.SemaphoreType.DMA((PIECES + 2 + rows // BLOCK,)),
        ],
        flops=10 * rows * width * HEAD,
    )(
        core.reshape(1),
        weights,
        x,
        halo,
        cosine,
        sine,
        decay,
        column,
        keys,
        values,
        base,
        before,
        fade,
        conv_taps,
    )
    theirs = lax.ppermute(branches, "core", [(0, 1), (1, 0)])
    (partial,) = call(out_kernel, [fast((tp, own_rows, width), BF16)], "out", flops=rows * width * 4 * HEAD)(
        branches, theirs, out_weight
    )
    (mixed,) = call(sum_kernel, [slow((own_rows, width), BF16)], "sum")(exchanged(partial, "tp"))
    return mixed


def solution(mesh):
    groups, stretches, tp = mesh.devices.shape
    chips = stretches // 2
    fine = Mesh(
        mesh.devices.reshape(groups, chips // 4, 2, 2, 2, tp), ("grp", "za", "zb", "zc", "core", "tp")
    )
    columns = P(STRETCHES, "tp")
    placed = (
        P(("grp", *STRETCHES, "tp"), None),
        P(),
        *([columns] * 7),
        P(None, "tp"),
        P("tp", STRETCHES),
        P("tp", STRETCHES),
        P(("grp", *STRETCHES), "tp"),
    )
    return jax.shard_map(
        body, mesh=fine, in_specs=placed, out_specs=P(("grp", *STRETCHES, "tp"), None), check_vma=False
    )
```

```python
import jax
import jax.numpy as jnp
from jax import lax
from jax.experimental import pallas as pl
from jax.experimental.pallas import tpu as pltpu
from jax.sharding import Mesh, PartitionSpec as P

HEAD = 128
HALF = HEAD // 2
CONV_K = 3
EPSILON = 1e-06
ROTARY_BASE = 10000.0
BLOCK = 256
EXTRA = 8
RIM = 16
PROJECTED = 5 * HEAD
PIECES = 4
COLUMNS = 7 * HEAD
INTERPRET = False

BF16 = jnp.bfloat16
F32 = jnp.float32
CHIPS = ("za", "zb", "zc")
STRETCHES = ("za", "zb", "zc", "core")
NEAR = ("zb", "zc")
FAR = ("za", "zb")

VMEM = pl.BlockSpec(memory_space=pltpu.VMEM)
PLAIN = pl.BlockSpec(memory_space=pltpu.VMEM)
SMEM = pl.BlockSpec(memory_space=pltpu.SMEM)
ANY = pl.BlockSpec(memory_space=pl.ANY)


def call(kernel, outs, name, specs=None, scratch=(), flops=0, limit=16):
    def run(*args):
        in_specs = specs if specs is not None else [VMEM] * len(args)
        placed = [placed_for(arg, spec) for arg, spec in zip(args, in_specs)]
        return pl.pallas_call(
            kernel,
            out_shape=[o[0] for o in outs],
            in_specs=in_specs,
            out_specs=[o[1] for o in outs],
            scratch_shapes=list(scratch),
            interpret=INTERPRET,
            name=name,
            compiler_params=pltpu.CompilerParams(vmem_limit_bytes=limit << 20 if limit else None),
            cost_estimate=pl.CostEstimate(flops=flops, bytes_accessed=0, transcendentals=0),
        )(*placed)

    return run


def placed_for(arg, spec):
    if INTERPRET or all(spec is not kind for kind in (VMEM, ANY)):
        return arg
    return pltpu.with_memory_space_constraint(arg, pltpu.VMEM if spec is VMEM else pltpu.HBM)


def fast(dims, kind):
    return (jax.ShapeDtypeStruct(dims, kind) if INTERPRET else pltpu.VMEM(dims, kind), VMEM)


def slow(dims, kind):
    return (jax.ShapeDtypeStruct(dims, kind), VMEM)


def dot(a, b, dims):
    return lax.dot_general(a, b, (dims, ((), ())), preferred_element_type=F32)


def pack_kernel(key, value, *refs):
    *inputs, logs, rest, message = refs
    for at, ref in enumerate(inputs):
        for core in range(2):
            to = core * COLUMNS + at * HEAD
            rest[:, to : to + HEAD] = ref[:, core * HEAD : (core + 1) * HEAD]
    shard = key.shape[0]
    for core in range(2):
        message[core, :shard, :HEAD] = key[:, core * HEAD : (core + 1) * HEAD]
        message[core, :shard, HEAD:] = value[:, core * HEAD : (core + 1) * HEAD]
        lines = [logs[core : core + 1, at : at + 2 * HEAD] for at in range(0, logs.shape[1], 2 * HEAD)]
        line = jnp.concatenate(lines, axis=0)
        high = line.astype(BF16).astype(F32)
        middle = (line - high).astype(BF16).astype(F32)
        low = line - high - middle
        filler = jnp.zeros((EXTRA - 3 * len(lines), 2 * HEAD), F32)
        message[core, shard:, :] = jnp.concatenate([high, middle, low, filler], axis=0).astype(BF16)


def logs_of(rows, lines):
    rows = rows.astype(F32)
    return rows[:lines] + rows[lines : 2 * lines] + rows[2 * lines : 3 * lines]


def norm_kernel(tokens, gain, out):
    values = tokens[...].astype(F32)
    scale = lax.rsqrt(jnp.mean(values * values, axis=-1, keepdims=True) + EPSILON)
    normed = (values * scale * gain[...].astype(F32)[None, :]).astype(BF16)
    for copy in range(out.shape[0]):
        out[copy] = normed


def rotated(head, cosine, sine):
    return head * cosine + pltpu.roll(head, HALF, 1) * sine


def table(i, cos_far, sin_far, cos_near, sin_near):
    cos_at = cos_far[i : i + 1, :] * cos_near[...] - sin_far[i : i + 1, :] * sin_near[...]
    sin_at = sin_far[i : i + 1, :] * cos_near[...] + cos_far[i : i + 1, :] * sin_near[...]
    first = lax.broadcasted_iota(jnp.int32, sin_at.shape, 1) < HALF
    return cos_at, jnp.where(first, -sin_at, sin_at)


def kv_kernel(
    pair, x, same, low, high, own, cos_far, sin_far, cos_near, sin_near, k_out, v_out, decay, column, totals, message, last, x_early, x_late, weight, semaphores
):
    per = BLOCK // x.shape[1]
    early = x_early.shape[0] // per
    copies = [
        pltpu.make_async_copy(
            x.at[pl.ds(i * per, per)],
            (x_early.at[pl.ds(i * per, per)] if i < early else x_late.at[pl.ds((i - early) * per, per)]),
            semaphores.at[i],
        )
        for i in range(x.shape[0] // per)
    ]
    for copy in copies:
        copy.start()
    rows, width = x.shape[0] * x.shape[1], x.shape[2]
    half = low.shape[0]
    shard = own.shape[1] - EXTRA
    lines = rows // 2 // (2 * HEAD)

    pieces = []
    for core in range(2):
        logs = logs_of(own[core, shard:, :], lines)
        for line in range(lines):
            pieces += [logs[line : line + 1, :HEAD], logs[line : line + 1, HEAD:]]
    logs = jnp.concatenate(pieces, axis=0)
    upper = lax.broadcasted_iota(jnp.int32, (HEAD, HEAD), 0) <= lax.broadcasted_iota(jnp.int32, (HEAD, HEAD), 1)
    inner = lax.dot_general(
        logs,
        upper.astype(F32),
        (((1,), (0,)), ((), ())),
        precision=lax.Precision.HIGHEST,
        preferred_element_type=F32,
    )
    before = jnp.zeros((1, 1), F32)
    added = []
    for at in range(len(pieces)):
        added.append(inner[at : at + 1] + before)
        before = before + inner[at : at + 1, HEAD - 1 :]
    cumulative = jnp.concatenate(added, axis=0)
    decay[...] = cumulative
    filler = jnp.zeros((HEAD - len(pieces), HEAD), F32)
    column[...] = jnp.concatenate([cumulative, filler], axis=0).T
    total = before

    mine, others = pair[0], 1 - pair[0]
    for source, first, place in ((same, 0, mine), (low, 0, others), (high, half, others)):
        for at_far in range(source.shape[0]):
            chip = 2 * (first + at_far) + place
            log_total = jnp.zeros((1, 1), F32)
            for core in range(2):
                at = core * (shard + EXTRA)
                to = pl.multiple_of((2 * chip + core) * shard, shard)
                weight[pl.ds(to, shard), :] = source[at_far, at : at + shard, :]
                logs = logs_of(source[at_far, at + shard : at + shard + EXTRA, :], lines)
                log_total = log_total + jnp.sum(logs, axis=(0, 1), keepdims=True)
            totals[pl.ds(chip, 1), :] = jnp.broadcast_to(log_total, (1, HEAD))

    state = jnp.zeros((HEAD, HEAD), F32)
    for i in range(rows // BLOCK):
        at = pl.ds(i * BLOCK, BLOCK)
        cos_at, sin_at = table(i, cos_far, sin_far, cos_near, sin_near)
        copies[i].wait()
        both = dot(block_rows(x_early, i) if i < early else block_rows(x_late, i - early), weight[...], ((1,), (0,))).astype(BF16)
        key = rotated(both[:, :HEAD].astype(F32), cos_at, sin_at) * HEAD ** (-0.5)
        k_out[at, :] = key.astype(BF16)
        value = both[:, HEAD:]
        v_out[at, :] = value
        here = block_column(column, i)
        faded = (key * jnp.exp(total - here)).astype(BF16)
        state = state + dot(faded, value, ((0,), (0,)))
    for copy in range(message.shape[0]):
        message[copy] = state.astype(BF16)
    last[...] = x_late[x_late.shape[0] - 1, x.shape[1] - RIM :, :]


def block_rows(x, i):
    per = BLOCK // x.shape[1]
    return x[i * per : (i + 1) * per].reshape(BLOCK, x.shape[2])


def block_column(column, i):
    per = BLOCK // HEAD
    return jnp.concatenate([column[:, per * i + j : per * i + j + 1] for j in range(per)], axis=0)


def near_kernel(place, block, totals, gathered, message, before, fade, scratch):
    own = place[0]
    near = gathered.shape[0]
    run = jnp.zeros((HEAD, HEAD), F32)
    passed = jnp.zeros((1, HEAD), F32)
    kept, kept_passed = run, passed
    for at in range(near):
        kept = jnp.where(own == at, run, kept)
        kept_passed = jnp.where(own == at, passed, kept_passed)
        log_total = totals[pl.ds(block[0] * near + at, 1), :]
        run = jnp.exp(log_total) * run + gathered[at].astype(F32)
        passed = passed + log_total
    before[...] = kept
    fade[...] = jnp.broadcast_to(jnp.exp(kept_passed), fade.shape)
    scratch[...] = run
    share = HEAD // near
    part = scratch[pl.ds(pl.multiple_of(own * share, share), share), :].astype(BF16)
    for copy in range(message.shape[0]):
        message[copy] = part


def far_kernel(place, totals, gathered, message):
    own = place[0]
    near, share = message.shape[:2]
    run = jnp.zeros((share, HEAD), F32)
    kept = run
    for at in range(gathered.shape[0]):
        kept = jnp.where(own == at, run, kept)
        log_total = jnp.sum(totals[at * near : (at + 1) * near, :], axis=0, keepdims=True)
        run = jnp.exp(log_total) * run + gathered[at].astype(F32)
    for copy in range(near):
        message[copy] = kept.astype(BF16)


def branch_kernel(
    core,
    weights,
    x_far,
    x_early,
    halo,
    cos_far,
    sin_far,
    cos_near,
    sin_near,
    decay,
    column,
    keys,
    values,
    base,
    before,
    fade,
    taps,
    branches,
    x_late,
    weight,
    semaphores,
):
    rows = x_far.shape[0] * x_far.shape[1]
    blocks = rows // BLOCK
    own = core[0]
    start_at = pl.multiple_of(own * COLUMNS, HEAD)
    piece = weight.shape[0] // PIECES
    copies = [
        *(
            pltpu.make_async_copy(
                weights.at[pl.ds(at, piece), pl.ds(start_at, PROJECTED)],
                weight.at[pl.ds(at, piece), :],
                semaphores.at[at // piece],
            )
            for at in range(0, weight.shape[0], piece)
        ),
    ]
    per_block = x_far.shape[0] // blocks
    early = x_early.shape[0] // per_block
    x_copies = [
        pltpu.make_async_copy(
            x_far.at[pl.ds(i * per_block, per_block)],
            x_late.at[pl.ds((i - early) * per_block, per_block)],
            semaphores.at[PIECES + i - early],
        )
        for i in range(early, blocks)
    ]
    for copy in (*copies, *x_copies):
        copy.start()
    incoming = jnp.concatenate([base[at].astype(F32) for at in range(base.shape[0])], axis=0)
    state = fade[0:1, :] * incoming + before[...]
    row = lax.broadcasted_iota(jnp.int32, (BLOCK, HEAD), 0)
    causal = lax.broadcasted_iota(jnp.int32, (BLOCK, BLOCK), 0) >= lax.broadcasted_iota(
        jnp.int32, (BLOCK, BLOCK), 1
    )
    tap = jnp.where(own == 0, taps[:, :HEAD].astype(F32), taps[:, HEAD:].astype(F32))
    start = jnp.zeros((1, 1), F32)
    per = BLOCK // HEAD
    first = jnp.zeros((BLOCK, PROJECTED), F32)
    for at in range(PIECES):
        copies[at].wait()
        cut = slice(at * piece, (at + 1) * piece)
        first = first + dot(block_rows(x_early, 0)[:, cut], weight[cut, :], ((1,), (0,)))
    rim = dot(halo[...], weight[:, HEAD : 3 * HEAD], ((1,), (0,))).astype(BF16).astype(F32)
    tail = (rim[:, :HEAD] * rim[:, HEAD:])[RIM - 8 :]
    for i in range(rows // BLOCK):
        at = pl.ds(i * BLOCK, BLOCK)
        half = (i * BLOCK) // (rows // 2)
        place = slice(i * BLOCK - half * (rows // 2), (i + 1) * BLOCK - half * (rows // 2))
        slot = jnp.where(own == half, 0, 1)
        if i >= early:
            x_copies[i - early].wait()
        rows_at = block_rows(x_early, i) if i < early else block_rows(x_late, i - early)
        cos_at, sin_at = table(i, cos_far, sin_far, cos_near, sin_near)
        projected = (dot(rows_at, weight[...], ((1,), (0,))) if i else first).astype(BF16)
        outer = projected[:, :HEAD].astype(F32)
        mixed = projected[:, HEAD : 2 * HEAD].astype(F32) * projected[:, 2 * HEAD : 3 * HEAD].astype(F32)
        one = jnp.where(row == 0, tail[7:8], pltpu.roll(mixed, 1, 0))
        two = jnp.where(row == 0, tail[6:7], jnp.where(row == 1, tail[7:8], pltpu.roll(mixed, 2, 0)))
        conv = tap[0:1] * two + tap[1:2] * one + tap[2:3] * mixed
        tail = mixed[BLOCK - 8 :]
        branches[slot, place, :HEAD] = (outer * conv).astype(BF16)

        query = rotated(projected[:, 3 * HEAD : 4 * HEAD].astype(F32), cos_at, sin_at)
        query = query.astype(BF16)
        key, value = keys[at, :], values[at, :]
        here = block_column(column, i)
        line = jnp.concatenate([decay[per * i + j : per * i + j + 1, :] for j in range(per)], axis=1)
        spread = jnp.where(causal, here - line, 0.0)
        scores = jnp.where(causal, dot(query, key, ((1,), (1,))) * jnp.exp(spread), 0.0)
        within = dot(scores.astype(BF16), value, ((1,), (0,)))
        across = dot(query, state.astype(BF16), ((1,), (0,))) * jnp.exp(here - start)
        retained = within + across
        end = line[:, BLOCK - 1 :]
        faded = (key.astype(F32) * jnp.exp(end - here)).astype(BF16)
        state = jnp.exp(end - start) * state + dot(faded, value, ((0,), (0,)))
        start = end
        normed = retained * lax.rsqrt(jnp.mean(retained * retained, axis=-1, keepdims=True) + EPSILON)
        gate = projected[:, 4 * HEAD :].astype(F32)
        ret_branch = (normed * (gate / (1.0 + jnp.exp(-gate)))).astype(BF16)

        branches[slot, place, HEAD:] = ret_branch


def fetch_kernel(core, weights, after, out, semaphores):
    del after
    own = core[0]
    copies = []
    for side, half in enumerate((own, 1 - own)):
        at = pl.multiple_of(half * COLUMNS + PROJECTED, HEAD)
        copies.append(
            pltpu.make_async_copy(weights.at[:, pl.ds(at, 2 * HEAD)], out.at[side], semaphores.at[side])
        )
    for copy in copies:
        copy.start()
    for copy in copies:
        copy.wait()


def out_kernel(mine, theirs, weight, out):
    parts, rows = out.shape[0], out.shape[1]
    step = 512
    for column in range(0, out.shape[2], step):
        at = pl.ds(column, step)
        total = dot(mine[0], weight[0, at, :], ((1,), (1,))) + dot(theirs[1], weight[1, at, :], ((1,), (1,)))
        total = total.astype(BF16)
        for part in range(parts):
            out[part, :, column : column + step] = total[part * rows : (part + 1) * rows]


def sum_kernel(parts, out):
    total = parts[0].astype(F32)
    for at in range(1, parts.shape[0]):
        total = total + parts[at].astype(F32)
    out[...] = total.astype(BF16)


def exchanged(x, axes):
    return lax.all_to_all(x, axes, 0, 0, tiled=True)


def body(
    tokens,
    norm_gain,
    conv_outer_weight,
    conv_inner_weight,
    conv_input_weight,
    query_matrix,
    key_weight,
    value_weight,
    gate_weight,
    conv_taps,
    conv_out_weight,
    ret_out_weight,
    log_decay,
):
    own_rows, width = tokens.shape
    tp = lax.axis_size("tp")
    chip = lax.axis_index(CHIPS)
    core = lax.axis_index("core")
    chips = lax.axis_size(CHIPS)
    near, far = lax.axis_size(NEAR), lax.axis_size("za")
    rows = 2 * tp * own_rows
    shard = key_weight.shape[0]

    rest, message = call(
        pack_kernel,
        [slow((shard, 2 * COLUMNS), BF16), fast((2, shard + EXTRA, 2 * HEAD), BF16)],
        "pack",
        specs=[PLAIN] * 10,
        limit=None,
    )(
        key_weight,
        value_weight,
        conv_outer_weight,
        conv_inner_weight,
        conv_input_weight,
        query_matrix,
        gate_weight,
        conv_out_weight.T,
        ret_out_weight.T,
        log_decay.T,
    )
    weights = lax.all_gather(rest, STRETCHES, axis=0, tiled=True)

    own = exchanged(message, "core")
    same = lax.all_gather(own.reshape(2 * (shard + EXTRA), 2 * HEAD), FAR)
    half = same.shape[0] // 2
    low = lax.ppermute(same[:half], CHIPS, [(i, (i - 1) % chips) for i in range(chips)])
    high = lax.ppermute(same[half:], CHIPS, [(i, (i + 1) % chips) for i in range(chips)])

    (normed,) = call(norm_kernel, [slow((2 * tp, own_rows, width), BF16)], "norm", specs=[PLAIN] * 2, limit=None)(
        tokens, norm_gain
    )
    x = exchanged(normed, ("core", "tp"))

    inv_freq = ROTARY_BASE ** (-jnp.arange(HALF, dtype=F32) / HALF)
    inv_freq = jnp.concatenate([inv_freq, inv_freq])[None, :]
    far_angle = ((chip * rows).astype(F32) + BLOCK * jnp.arange(8, dtype=F32))[:, None] * inv_freq
    near_angle = jnp.arange(BLOCK, dtype=F32)[:, None] * inv_freq
    tables = (jnp.cos(far_angle), jnp.sin(far_angle), jnp.cos(near_angle), jnp.sin(near_angle))

    held = BLOCK // own_rows
    keys, values, decay, column, totals, message, last, x_early = call(
        kv_kernel,
        [
            fast((rows, HEAD), BF16),
            fast((rows, HEAD), BF16),
            fast((rows // HEAD, HEAD), F32),
            fast((HEAD, HEAD), F32),
            fast((chips, HEAD), F32),
            fast((near, HEAD, HEAD), BF16),
            fast((RIM, width), BF16),
            fast((held, own_rows, width), BF16),
        ],
        "kv",
        specs=[SMEM, ANY] + [VMEM] * 8,
        scratch=[
            pltpu.VMEM((2 * tp - held, own_rows, width), BF16),
            pltpu.VMEM((width, 2 * HEAD), BF16),
            pltpu.SemaphoreType.DMA((rows // BLOCK,)),
        ],
        flops=4 * rows * width * HEAD,
    )(lax.axis_index("zc").reshape(1), x, same, low, high, own, *tables)

    halo = lax.ppermute(last, CHIPS, [(i, i + 1) for i in range(chips - 1)])

    share = HEAD // near
    block = lax.axis_index("za").reshape(1)
    message, before, fade = call(
        near_kernel,
        [fast((far, share, HEAD), BF16), fast((HEAD, HEAD), F32), fast((8, HEAD), F32)],
        "near",
        specs=[SMEM, SMEM, VMEM, VMEM],
        scratch=[pltpu.VMEM((HEAD, HEAD), F32)],
    )(lax.axis_index(NEAR).reshape(1), block, totals, exchanged(message, NEAR))
    (message,) = call(far_kernel, [fast((near, share, HEAD), BF16)], "far", specs=[SMEM, VMEM, VMEM])(
        block, totals, exchanged(message, "za")
    )
    base = exchanged(message, NEAR)

    (branches,) = call(
        branch_kernel,
        [fast((2, rows // 2, 2 * HEAD), BF16)],
        "branch",
        specs=[SMEM, ANY, ANY] + [VMEM] * 14,
        scratch=[
            pltpu.VMEM((2 * tp - held, own_rows, width), BF16),
            pltpu.VMEM((width, PROJECTED), BF16),
            pltpu.SemaphoreType.DMA((PIECES + rows // BLOCK,)),
        ],
        flops=10 * rows * width * HEAD,
    )(
        core.reshape(1),
        weights,
        x,
        x_early,
        halo,
        *tables,
        decay,
        column,
        keys,
        values,
        base,
        before,
        fade,
        conv_taps,
    )
    theirs = lax.ppermute(branches, "core", [(0, 1), (1, 0)])
    (out_weight,) = call(
        fetch_kernel,
        [fast((2, width, 2 * HEAD), BF16)],
        "fetch",
        specs=[SMEM, ANY, VMEM],
        scratch=[pltpu.SemaphoreType.DMA((2,))],
        flops=1 << 28,
    )(core.reshape(1), weights, branches)
    (partial,) = call(out_kernel, [fast((tp, own_rows, width), BF16)], "out", flops=rows * width * 4 * HEAD)(
        branches, theirs, out_weight
    )
    (mixed,) = call(sum_kernel, [slow((own_rows, width), BF16)], "sum")(exchanged(partial, "tp"))
    return mixed


def solution(mesh):
    groups, stretches, tp = mesh.devices.shape
    chips = stretches // 2
    fine = Mesh(
        mesh.devices.reshape(groups, chips // 4, 2, 2, 2, tp), ("grp", "za", "zb", "zc", "core", "tp")
    )
    columns = P(STRETCHES, "tp")
    placed = (
        P(("grp", *STRETCHES, "tp"), None),
        P(),
        *([columns] * 7),
        P(None, "tp"),
        P("tp", STRETCHES),
        P("tp", STRETCHES),
        P(("grp", *STRETCHES), "tp"),
    )
    return jax.shard_map(
        body, mesh=fine, in_specs=placed, out_specs=P(("grp", *STRETCHES, "tp"), None), check_vma=False
    )
```

```python
import jax
import jax.numpy as jnp
from jax import lax
from jax.experimental import pallas as pl
from jax.experimental.pallas import tpu as pltpu
from jax.sharding import Mesh, PartitionSpec as P

HEAD = 128
HALF = HEAD // 2
CONV_K = 3
EPSILON = 1e-06
ROTARY_BASE = 10000.0
BLOCK = 256
EXTRA = 8
RIM = 16
PROJECTED = 5 * HEAD
PIECES = 4
COLUMNS = 7 * HEAD
INTERPRET = False

BF16 = jnp.bfloat16
F32 = jnp.float32
CHIPS = ("za", "zb", "zc")
STRETCHES = ("za", "zb", "zc", "core")
NEAR = ("zb", "zc")
FAR = ("za", "zb")

VMEM = pl.BlockSpec(memory_space=pltpu.VMEM)
PLAIN = pl.BlockSpec(memory_space=pltpu.VMEM)
SMEM = pl.BlockSpec(memory_space=pltpu.SMEM)
ANY = pl.BlockSpec(memory_space=pl.ANY)


def call(kernel, outs, name, specs=None, scratch=(), flops=0, limit=16):
    def run(*args):
        in_specs = specs if specs is not None else [VMEM] * len(args)
        placed = [placed_for(arg, spec) for arg, spec in zip(args, in_specs)]
        return pl.pallas_call(
            kernel,
            out_shape=[o[0] for o in outs],
            in_specs=in_specs,
            out_specs=[o[1] for o in outs],
            scratch_shapes=list(scratch),
            interpret=INTERPRET,
            name=name,
            compiler_params=pltpu.CompilerParams(vmem_limit_bytes=limit << 20 if limit else None),
            cost_estimate=pl.CostEstimate(flops=flops, bytes_accessed=0, transcendentals=0),
        )(*placed)

    return run


def placed_for(arg, spec):
    if INTERPRET or all(spec is not kind for kind in (VMEM, ANY)):
        return arg
    return pltpu.with_memory_space_constraint(arg, pltpu.VMEM if spec is VMEM else pltpu.HBM)


def fast(dims, kind):
    return (jax.ShapeDtypeStruct(dims, kind) if INTERPRET else pltpu.VMEM(dims, kind), VMEM)


def slow(dims, kind):
    return (jax.ShapeDtypeStruct(dims, kind), VMEM)


def dot(a, b, dims):
    return lax.dot_general(a, b, (dims, ((), ())), preferred_element_type=F32)


def pack_kernel(key, value, *refs):
    *inputs, logs, rest, message = refs
    for at, ref in enumerate(inputs):
        for core in range(2):
            to = core * COLUMNS + at * HEAD
            rest[:, to : to + HEAD] = ref[:, core * HEAD : (core + 1) * HEAD]
    shard = key.shape[0]
    for core in range(2):
        message[core, :shard, :HEAD] = key[:, core * HEAD : (core + 1) * HEAD]
        message[core, :shard, HEAD:] = value[:, core * HEAD : (core + 1) * HEAD]
        lines = [logs[core : core + 1, at : at + 2 * HEAD] for at in range(0, logs.shape[1], 2 * HEAD)]
        line = jnp.concatenate(lines, axis=0)
        high = line.astype(BF16).astype(F32)
        middle = (line - high).astype(BF16).astype(F32)
        low = line - high - middle
        filler = jnp.zeros((EXTRA - 3 * len(lines), 2 * HEAD), F32)
        message[core, shard:, :] = jnp.concatenate([high, middle, low, filler], axis=0).astype(BF16)


def logs_of(rows, lines):
    rows = rows.astype(F32)
    return rows[:lines] + rows[lines : 2 * lines] + rows[2 * lines : 3 * lines]


def norm_kernel(tokens, gain, out):
    values = tokens[...].astype(F32)
    scale = lax.rsqrt(jnp.mean(values * values, axis=-1, keepdims=True) + EPSILON)
    normed = (values * scale * gain[...].astype(F32)[None, :]).astype(BF16)
    for copy in range(out.shape[0]):
        out[copy] = normed


def rotated(head, cosine, sine):
    return head * cosine + pltpu.roll(head, HALF, 1) * sine


def table(i, cos_far, sin_far, cos_near, sin_near):
    cos_at = cos_far[i : i + 1, :] * cos_near[...] - sin_far[i : i + 1, :] * sin_near[...]
    sin_at = sin_far[i : i + 1, :] * cos_near[...] + cos_far[i : i + 1, :] * sin_near[...]
    first = lax.broadcasted_iota(jnp.int32, sin_at.shape, 1) < HALF
    return cos_at, jnp.where(first, -sin_at, sin_at)


def kv_kernel(
    pair, x, same, low, high, own, cos_far, sin_far, cos_near, sin_near, k_out, v_out, decay, column, totals, message, last, x_early, x_late, weight, semaphores
):
    per = BLOCK // x.shape[1]
    early = x_early.shape[0] // per
    copies = [
        pltpu.make_async_copy(
            x.at[pl.ds(i * per, per)],
            (x_early.at[pl.ds(i * per, per)] if i < early else x_late.at[pl.ds((i - early) * per, per)]),
            semaphores.at[i],
        )
        for i in range(x.shape[0] // per)
    ]
    for copy in copies:
        copy.start()
    rows, width = x.shape[0] * x.shape[1], x.shape[2]
    half = low.shape[0]
    shard = own.shape[1] - EXTRA
    lines = rows // 2 // (2 * HEAD)

    pieces = []
    for core in range(2):
        logs = logs_of(own[core, shard:, :], lines)
        for line in range(lines):
            pieces += [logs[line : line + 1, :HEAD], logs[line : line + 1, HEAD:]]
    logs = jnp.concatenate(pieces, axis=0)
    upper = lax.broadcasted_iota(jnp.int32, (HEAD, HEAD), 0) <= lax.broadcasted_iota(jnp.int32, (HEAD, HEAD), 1)
    inner = lax.dot_general(
        logs,
        upper.astype(F32),
        (((1,), (0,)), ((), ())),
        precision=lax.Precision.HIGHEST,
        preferred_element_type=F32,
    )
    before = jnp.zeros((1, 1), F32)
    added = []
    for at in range(len(pieces)):
        added.append(inner[at : at + 1] + before)
        before = before + inner[at : at + 1, HEAD - 1 :]
    cumulative = jnp.concatenate(added, axis=0)
    decay[...] = cumulative
    filler = jnp.zeros((HEAD - len(pieces), HEAD), F32)
    column[...] = jnp.concatenate([cumulative, filler], axis=0).T
    total = before

    mine, others = pair[0], 1 - pair[0]
    for source, first, place in ((same, 0, mine), (low, 0, others), (high, half, others)):
        for at_far in range(source.shape[0]):
            chip = 2 * (first + at_far) + place
            log_total = jnp.zeros((1, 1), F32)
            for core in range(2):
                at = core * (shard + EXTRA)
                to = pl.multiple_of((2 * chip + core) * shard, shard)
                weight[pl.ds(to, shard), :] = source[at_far, at : at + shard, :]
                logs = logs_of(source[at_far, at + shard : at + shard + EXTRA, :], lines)
                log_total = log_total + jnp.sum(logs, axis=(0, 1), keepdims=True)
            totals[pl.ds(chip, 1), :] = jnp.broadcast_to(log_total, (1, HEAD))

    state = jnp.zeros((HEAD, HEAD), F32)
    for i in range(rows // BLOCK):
        at = pl.ds(i * BLOCK, BLOCK)
        cos_at, sin_at = table(i, cos_far, sin_far, cos_near, sin_near)
        copies[i].wait()
        both = dot(block_rows(x_early, i) if i < early else block_rows(x_late, i - early), weight[...], ((1,), (0,))).astype(BF16)
        key = rotated(both[:, :HEAD].astype(F32), cos_at, sin_at) * HEAD ** (-0.5)
        k_out[at, :] = key.astype(BF16)
        value = both[:, HEAD:]
        v_out[at, :] = value
        here = block_column(column, i)
        faded = (key * jnp.exp(total - here)).astype(BF16)
        state = state + dot(faded, value, ((0,), (0,)))
    for copy in range(message.shape[0]):
        message[copy] = state.astype(BF16)
    last[...] = x_late[x_late.shape[0] - 1, x.shape[1] - RIM :, :]


def block_rows(x, i):
    per = BLOCK // x.shape[1]
    return x[i * per : (i + 1) * per].reshape(BLOCK, x.shape[2])


def block_column(column, i):
    per = BLOCK // HEAD
    return jnp.concatenate([column[:, per * i + j : per * i + j + 1] for j in range(per)], axis=0)


def near_kernel(place, block, totals, gathered, message, before, fade, scratch):
    own = place[0]
    near = gathered.shape[0]
    run = jnp.zeros((HEAD, HEAD), F32)
    passed = jnp.zeros((1, HEAD), F32)
    kept, kept_passed = run, passed
    for at in range(near):
        kept = jnp.where(own == at, run, kept)
        kept_passed = jnp.where(own == at, passed, kept_passed)
        log_total = totals[pl.ds(block[0] * near + at, 1), :]
        run = jnp.exp(log_total) * run + gathered[at].astype(F32)
        passed = passed + log_total
    before[...] = kept
    fade[...] = jnp.broadcast_to(jnp.exp(kept_passed), fade.shape)
    scratch[...] = run
    share = HEAD // near
    part = scratch[pl.ds(pl.multiple_of(own * share, share), share), :].astype(BF16)
    for copy in range(message.shape[0]):
        message[copy] = part


def far_kernel(place, totals, gathered, message):
    own = place[0]
    near, share = message.shape[:2]
    run = jnp.zeros((share, HEAD), F32)
    kept = run
    for at in range(gathered.shape[0]):
        kept = jnp.where(own == at, run, kept)
        log_total = jnp.sum(totals[at * near : (at + 1) * near, :], axis=0, keepdims=True)
        run = jnp.exp(log_total) * run + gathered[at].astype(F32)
    for copy in range(near):
        message[copy] = kept.astype(BF16)


def branch_kernel(
    core,
    weights,
    x_far,
    x_early,
    halo,
    cos_far,
    sin_far,
    cos_near,
    sin_near,
    decay,
    column,
    keys,
    values,
    base,
    before,
    fade,
    taps,
    branches,
    x_late,
    weight,
    semaphores,
):
    rows = x_far.shape[0] * x_far.shape[1]
    blocks = rows // BLOCK
    own = core[0]
    start_at = pl.multiple_of(own * COLUMNS, HEAD)
    piece = weight.shape[0] // PIECES
    copies = [
        *(
            pltpu.make_async_copy(
                weights.at[pl.ds(at, piece), pl.ds(start_at, PROJECTED)],
                weight.at[pl.ds(at, piece), :],
                semaphores.at[at // piece],
            )
            for at in range(0, weight.shape[0], piece)
        ),
    ]
    per_block = x_far.shape[0] // blocks
    early = x_early.shape[0] // per_block
    x_copies = [
        pltpu.make_async_copy(
            x_far.at[pl.ds(i * per_block, per_block)],
            x_late.at[pl.ds((i - early) * per_block, per_block)],
            semaphores.at[PIECES + i - early],
        )
        for i in range(early, blocks)
    ]
    for copy in copies:
        copy.start()
    incoming = jnp.concatenate([base[at].astype(F32) for at in range(base.shape[0])], axis=0)
    state = fade[0:1, :] * incoming + before[...]
    row = lax.broadcasted_iota(jnp.int32, (BLOCK, HEAD), 0)
    causal = lax.broadcasted_iota(jnp.int32, (BLOCK, BLOCK), 0) >= lax.broadcasted_iota(
        jnp.int32, (BLOCK, BLOCK), 1
    )
    tap = jnp.where(own == 0, taps[:, :HEAD].astype(F32), taps[:, HEAD:].astype(F32))
    start = jnp.zeros((1, 1), F32)
    per = BLOCK // HEAD
    first = jnp.zeros((BLOCK, PROJECTED), F32)
    for at in range(PIECES):
        copies[at].wait()
        if at == PIECES // 2:
            x_copies[0].start()
        cut = slice(at * piece, (at + 1) * piece)
        first = first + dot(block_rows(x_early, 0)[:, cut], weight[cut, :], ((1,), (0,)))
    for copy in x_copies[1:]:
        copy.start()
    rim = dot(halo[...], weight[:, HEAD : 3 * HEAD], ((1,), (0,))).astype(BF16).astype(F32)
    tail = (rim[:, :HEAD] * rim[:, HEAD:])[RIM - 8 :]
    for i in range(rows // BLOCK):
        at = pl.ds(i * BLOCK, BLOCK)
        half = (i * BLOCK) // (rows // 2)
        place = slice(i * BLOCK - half * (rows // 2), (i + 1) * BLOCK - half * (rows // 2))
        slot = jnp.where(own == half, 0, 1)
        if i >= early:
            x_copies[i - early].wait()
        rows_at = block_rows(x_early, i) if i < early else block_rows(x_late, i - early)
        cos_at, sin_at = table(i, cos_far, sin_far, cos_near, sin_near)
        projected = (dot(rows_at, weight[...], ((1,), (0,))) if i else first).astype(BF16)
        outer = projected[:, :HEAD].astype(F32)
        mixed = projected[:, HEAD : 2 * HEAD].astype(F32) * projected[:, 2 * HEAD : 3 * HEAD].astype(F32)
        one = jnp.where(row == 0, tail[7:8], pltpu.roll(mixed, 1, 0))
        two = jnp.where(row == 0, tail[6:7], jnp.where(row == 1, tail[7:8], pltpu.roll(mixed, 2, 0)))
        conv = tap[0:1] * two + tap[1:2] * one + tap[2:3] * mixed
        tail = mixed[BLOCK - 8 :]
        branches[slot, place, :HEAD] = (outer * conv).astype(BF16)

        query = rotated(projected[:, 3 * HEAD : 4 * HEAD].astype(F32), cos_at, sin_at)
        query = query.astype(BF16)
        key, value = keys[at, :], values[at, :]
        here = block_column(column, i)
        line = jnp.concatenate([decay[per * i + j : per * i + j + 1, :] for j in range(per)], axis=1)
        spread = jnp.where(causal, here - line, 0.0)
        scores = jnp.where(causal, dot(query, key, ((1,), (1,))) * jnp.exp(spread), 0.0)
        within = dot(scores.astype(BF16), value, ((1,), (0,)))
        across = dot(query, state.astype(BF16), ((1,), (0,))) * jnp.exp(here - start)
        retained = within + across
        end = line[:, BLOCK - 1 :]
        faded = (key.astype(F32) * jnp.exp(end - here)).astype(BF16)
        state = jnp.exp(end - start) * state + dot(faded, value, ((0,), (0,)))
        start = end
        normed = retained * lax.rsqrt(jnp.mean(retained * retained, axis=-1, keepdims=True) + EPSILON)
        gate = projected[:, 4 * HEAD :].astype(F32)
        ret_branch = (normed * (gate / (1.0 + jnp.exp(-gate)))).astype(BF16)

        branches[slot, place, HEAD:] = ret_branch


def fetch_kernel(core, weights, after, out, semaphores):
    del after
    own = core[0]
    copies = []
    for side, half in enumerate((own, 1 - own)):
        at = pl.multiple_of(half * COLUMNS + PROJECTED, HEAD)
        copies.append(
            pltpu.make_async_copy(weights.at[:, pl.ds(at, 2 * HEAD)], out.at[side], semaphores.at[side])
        )
    for copy in copies:
        copy.start()
    for copy in copies:
        copy.wait()


def out_kernel(mine, theirs, weight, out):
    parts, rows = out.shape[0], out.shape[1]
    step = 512
    for column in range(0, out.shape[2], step):
        at = pl.ds(column, step)
        total = dot(mine[0], weight[0, at, :], ((1,), (1,))) + dot(theirs[1], weight[1, at, :], ((1,), (1,)))
        total = total.astype(BF16)
        for part in range(parts):
            out[part, :, column : column + step] = total[part * rows : (part + 1) * rows]


def sum_kernel(parts, out):
    total = parts[0].astype(F32)
    for at in range(1, parts.shape[0]):
        total = total + parts[at].astype(F32)
    out[...] = total.astype(BF16)


def exchanged(x, axes):
    return lax.all_to_all(x, axes, 0, 0, tiled=True)


def body(
    tokens,
    norm_gain,
    conv_outer_weight,
    conv_inner_weight,
    conv_input_weight,
    query_matrix,
    key_weight,
    value_weight,
    gate_weight,
    conv_taps,
    conv_out_weight,
    ret_out_weight,
    log_decay,
):
    own_rows, width = tokens.shape
    tp = lax.axis_size("tp")
    chip = lax.axis_index(CHIPS)
    core = lax.axis_index("core")
    chips = lax.axis_size(CHIPS)
    near, far = lax.axis_size(NEAR), lax.axis_size("za")
    rows = 2 * tp * own_rows
    shard = key_weight.shape[0]

    rest, message = call(
        pack_kernel,
        [slow((shard, 2 * COLUMNS), BF16), fast((2, shard + EXTRA, 2 * HEAD), BF16)],
        "pack",
        specs=[PLAIN] * 10,
        limit=None,
    )(
        key_weight,
        value_weight,
        conv_outer_weight,
        conv_inner_weight,
        conv_input_weight,
        query_matrix,
        gate_weight,
        conv_out_weight.T,
        ret_out_weight.T,
        log_decay.T,
    )
    weights = lax.all_gather(rest, STRETCHES, axis=0, tiled=True)

    own = exchanged(message, "core")
    same = lax.all_gather(own.reshape(2 * (shard + EXTRA), 2 * HEAD), FAR)
    half = same.shape[0] // 2
    low = lax.ppermute(same[:half], CHIPS, [(i, (i - 1) % chips) for i in range(chips)])
    high = lax.ppermute(same[half:], CHIPS, [(i, (i + 1) % chips) for i in range(chips)])

    (normed,) = call(norm_kernel, [slow((2 * tp, own_rows, width), BF16)], "norm", specs=[PLAIN] * 2, limit=None)(
        tokens, norm_gain
    )
    x = exchanged(normed, ("core", "tp"))

    inv_freq = ROTARY_BASE ** (-jnp.arange(HALF, dtype=F32) / HALF)
    inv_freq = jnp.concatenate([inv_freq, inv_freq])[None, :]
    far_angle = ((chip * rows).astype(F32) + BLOCK * jnp.arange(8, dtype=F32))[:, None] * inv_freq
    near_angle = jnp.arange(BLOCK, dtype=F32)[:, None] * inv_freq
    tables = (jnp.cos(far_angle), jnp.sin(far_angle), jnp.cos(near_angle), jnp.sin(near_angle))

    held = BLOCK // own_rows
    keys, values, decay, column, totals, message, last, x_early = call(
        kv_kernel,
        [
            fast((rows, HEAD), BF16),
            fast((rows, HEAD), BF16),
            fast((rows // HEAD, HEAD), F32),
            fast((HEAD, HEAD), F32),
            fast((chips, HEAD), F32),
            fast((near, HEAD, HEAD), BF16),
            fast((RIM, width), BF16),
            fast((held, own_rows, width), BF16),
        ],
        "kv",
        specs=[SMEM, ANY] + [VMEM] * 8,
        scratch=[
            pltpu.VMEM((2 * tp - held, own_rows, width), BF16),
            pltpu.VMEM((width, 2 * HEAD), BF16),
            pltpu.SemaphoreType.DMA((rows // BLOCK,)),
        ],
        flops=4 * rows * width * HEAD,
    )(lax.axis_index("zc").reshape(1), x, same, low, high, own, *tables)

    halo = lax.ppermute(last, CHIPS, [(i, i + 1) for i in range(chips - 1)])

    share = HEAD // near
    block = lax.axis_index("za").reshape(1)
    message, before, fade = call(
        near_kernel,
        [fast((far, share, HEAD), BF16), fast((HEAD, HEAD), F32), fast((8, HEAD), F32)],
        "near",
        specs=[SMEM, SMEM, VMEM, VMEM],
        scratch=[pltpu.VMEM((HEAD, HEAD), F32)],
    )(lax.axis_index(NEAR).reshape(1), block, totals, exchanged(message, NEAR))
    (message,) = call(far_kernel, [fast((near, share, HEAD), BF16)], "far", specs=[SMEM, VMEM, VMEM])(
        block, totals, exchanged(message, "za")
    )
    base = exchanged(message, NEAR)

    (branches,) = call(
        branch_kernel,
        [fast((2, rows // 2, 2 * HEAD), BF16)],
        "branch",
        specs=[SMEM, ANY, ANY] + [VMEM] * 14,
        scratch=[
            pltpu.VMEM((2 * tp - held, own_rows, width), BF16),
            pltpu.VMEM((width, PROJECTED), BF16),
            pltpu.SemaphoreType.DMA((PIECES + rows // BLOCK,)),
        ],
        flops=10 * rows * width * HEAD,
    )(
        core.reshape(1),
        weights,
        x,
        x_early,
        halo,
        *tables,
        decay,
        column,
        keys,
        values,
        base,
        before,
        fade,
        conv_taps,
    )
    theirs = lax.ppermute(branches, "core", [(0, 1), (1, 0)])
    (out_weight,) = call(
        fetch_kernel,
        [fast((2, width, 2 * HEAD), BF16)],
        "fetch",
        specs=[SMEM, ANY, VMEM],
        scratch=[pltpu.SemaphoreType.DMA((2,))],
        flops=1 << 28,
    )(core.reshape(1), weights, branches)
    (partial,) = call(out_kernel, [fast((tp, own_rows, width), BF16)], "out", flops=rows * width * 4 * HEAD)(
        branches, theirs, out_weight
    )
    (mixed,) = call(sum_kernel, [slow((own_rows, width), BF16)], "sum")(exchanged(partial, "tp"))
    return mixed


def solution(mesh):
    groups, stretches, tp = mesh.devices.shape
    chips = stretches // 2
    fine = Mesh(
        mesh.devices.reshape(groups, chips // 4, 2, 2, 2, tp), ("grp", "za", "zb", "zc", "core", "tp")
    )
    columns = P(STRETCHES, "tp")
    placed = (
        P(("grp", *STRETCHES, "tp"), None),
        P(),
        *([columns] * 7),
        P(None, "tp"),
        P("tp", STRETCHES),
        P("tp", STRETCHES),
        P(("grp", *STRETCHES), "tp"),
    )
    return jax.shard_map(
        body, mesh=fine, in_specs=placed, out_specs=P(("grp", *STRETCHES, "tp"), None), check_vma=False
    )
```
